512 devices in a mesh: ep: 128 (over z, y, core), tp: 4 (over x).
Axes of the slice: x: 4, y: 8, z: 8, core: 2. Of those that a mesh axis runs over, the one named last changes fastest.
Arguments:
- tokens: bfloat16 [16384, 2048], P('ep'), may hold values from -6 to 6
- expert_ids: int32 [16384, 2], P('ep'), may hold values from 0 to 127, as said below
- route_weights: bfloat16 [16384, 2], P('ep'), may hold values from 0.099609375 to 1
- cotangent: bfloat16 [16384, 2048], P('ep'), may hold values from -3 to 3
- w_gate: bfloat16 [128, 2048, 512], P('ep', None, 'tp'), may hold values from -0.125 to 0.125
- w_up: bfloat16 [128, 2048, 512], P('ep', None, 'tp'), may hold values from -0.125 to 0.125
- w_down: bfloat16 [128, 512, 2048], P('ep', 'tp'), may hold values from -0.25 to 0.25
Outputs:
- token_grad: bfloat16 [16384, 2048], P('ep', 'tp')
- route_grad: bfloat16 [16384, 2], P('ep')
- grad_gate: bfloat16 [128, 2048, 512], P('ep', None, 'tp')
- grad_up: bfloat16 [128, 2048, 512], P('ep', None, 'tp')
- grad_down: bfloat16 [128, 512, 2048], P('ep', 'tp')
- gate_rows: float32 [128, 2048], P('ep')
- up_rows: float32 [128, 2048], P('ep')
- down_rows: float32 [128, 512], P('ep', 'tp')
The draws below stay inside these ranges and needn't reach their ends.
Inputs may be any that keep to these rules, and one draw needn't show every extreme that they name: `expert_ids`: each row names 2 different experts of one group: both lie in g * 32 to (g + 1) * 32 - 1 for the row's group g. In the rows of one device (aligned blocks of 128 rows) no expert is named more than 4 times, and in every block some expert is named exactly 4 times.
All inputs are finite; a program needn't handle non-finite values.
Results may differ from the reference program's by a relative error of at most 0.012.
Values may be sent and summed in bfloat16 or wider, within the bound.
A program may use at most 64 MiB of HBM per device.

```python
import jax
import jax.numpy as jnp
from jax import lax

D = 2048
F = 512
GROUPS = 4
TOPK = 2
TOK_DEV = 128
EXPERTS = 128
CAP = 4
TOKENS = 16384
N_EP = 128
N_TP = 4


def draw_expert_ids(key, part):
    per_group = EXPERTS // GROUPS
    blocks = TOKENS // TOK_DEV
    hot_group = jax.random.randint(jax.random.fold_in(key, 11), (), 0, GROUPS)
    hot_member = jax.random.randint(jax.random.fold_in(key, 12), (), 0, per_group)
    block_keys = jax.random.split(jax.random.fold_in(key, 13), blocks)
    group_ids = jnp.arange(GROUPS, dtype=jnp.int32)
    member_ids = jnp.arange(per_group, dtype=jnp.int32)

    def one_block(block_key):
        key_a, key_b, key_c, key_d, key_e = jax.random.split(block_key, 5)
        hot_size = jax.random.randint(key_a, (), max(CAP, TOK_DEV // 4), TOK_DEV // 2 + 1)
        remain = TOK_DEV - hot_size
        third = remain // 3
        jitter = remain // 8
        first_size = jax.random.randint(key_b, (), third - jitter, third + jitter + 1)
        second_size = jax.random.randint(key_c, (), third - jitter, third + jitter + 1)
        others = jnp.stack([first_size, second_size, remain - first_size - second_size])
        other_slot = jnp.minimum((group_ids - hot_group - 1) % GROUPS, 2)
        sizes = jnp.where(group_ids == hot_group, hot_size, others[other_slot]).astype(jnp.int32)
        ends = jnp.cumsum(sizes)
        starts = ends - sizes
        fill_step = jnp.maximum(jnp.minimum(CAP, sizes), 1)
        ranks = jax.random.permutation(key_d, TOK_DEV).astype(jnp.int32)
        member_group = jnp.sum((ranks[:, None] >= ends[None, :]).astype(jnp.int32), axis=1)
        inner = ranks - starts[member_group]
        count = sizes[member_group]
        stride = fill_step[member_group]
        scores = jax.random.randint(key_e, (GROUPS, per_group), 0, 1 << 20) * per_group + member_ids[None, :]
        pinned = (group_ids[:, None] == hot_group) & (member_ids[None, :] == hot_member)
        scores = jnp.where(pinned, -1, scores)
        ordering = jnp.argsort(scores, axis=1).astype(jnp.int32)
        first_pick = ordering[member_group, inner // stride]
        second_pick = ordering[member_group, (inner + count) // stride]
        base_ids = member_group * per_group
        return jnp.stack([base_ids + first_pick, base_ids + second_pick], axis=1)
    return jax.vmap(one_block)(block_keys).reshape(TOKENS, TOPK).astype(jnp.int32)


def block_levels(key, extent, pieces, least, largest):
    loudness = 1.0
    for position, parts in pieces:
        steps = jax.random.uniform(jax.random.fold_in(jax.random.fold_in(key, 6), position), (parts,), jnp.float32, least / len(pieces), largest / len(pieces))
        loudness = loudness * jnp.repeat(jnp.exp(steps), extent[position] // parts).reshape((-1,) + (1,) * (len(extent) - 1 - position))
    return loudness


def noise(rng, shape, spread, bound, cuts=(), kind=jnp.bfloat16):
    result = jax.random.normal(rng, shape, jnp.float32) * spread
    if len(cuts) > 0:
        result = block_levels(rng, shape, cuts, -0.22, 0.18) * result
    return jnp.clip(result, min=-bound, max=bound).astype(kind)


def setup_inputs(seed: int = 0) -> dict:
    streams_of = jax.random.split(jax.random.key(seed), 8)
    tokens = noise(streams_of[0], (TOKENS, D), 1.0, 6.0, ((0, 128),))
    expert_ids = draw_expert_ids(jax.random.fold_in(streams_of[7], 71), 0)
    route_weights = jnp.clip(0.099609375 + 0.9003906 * jax.random.uniform(streams_of[2], (TOKENS, TOPK), jnp.float32) ** block_levels(streams_of[2], (TOKENS, TOPK), ((0, 128),), -0.2, 0.2), 0.099609375, 1.0).astype(jnp.bfloat16)
    cotangent = noise(streams_of[3], (TOKENS, D), 0.5, 3.0, ((0, 128),))
    w_gate = noise(streams_of[4], (EXPERTS, D, F), D ** -0.5, 0.125, ((0, 128), (2, 4)))
    w_up = noise(streams_of[5], (EXPERTS, D, F), D ** -0.5, 0.125, ((0, 128), (2, 4)))
    w_down = noise(streams_of[6], (EXPERTS, F, D), F ** -0.5, 0.25, ((0, 128), (1, 4)))
    return {"tokens": tokens, "expert_ids": expert_ids, "route_weights": route_weights, "cotangent": cotangent, "w_gate": w_gate, "w_up": w_up, "w_down": w_down}


def reference(tokens, expert_ids, route_weights, cotangent, w_gate, w_up, w_down):
    assigns = TOKENS * TOPK
    slot_total = N_EP * CAP
    quarter = F // N_TP
    flat_ids = expert_ids.reshape(-1).astype(jnp.int32)
    weight_flat = jnp.concatenate([route_weights.reshape(-1).astype(jnp.float32), jnp.zeros((1,), jnp.float32)])
    rows_pad = jnp.concatenate([tokens, jnp.zeros((1, D), jnp.bfloat16)], axis=0)
    cot_pad = jnp.concatenate([cotangent, jnp.zeros((1, D), jnp.bfloat16)], axis=0)

    def per_expert(expert):
        picked = jnp.nonzero(flat_ids == expert, size=slot_total, fill_value=assigns)[0].astype(jnp.int32)
        holder = (picked // TOPK).astype(jnp.int32)
        slot_rows = rows_pad[holder]
        slot_cot = cot_pad[holder]
        slot_scale = weight_flat[picked]
        gate_cols = w_gate[expert]
        up_cols = w_up[expert]
        down_rows_w = w_down[expert]
        gate_pre = jnp.dot(slot_rows, gate_cols, preferred_element_type=jnp.float32)
        up_pre = jnp.dot(slot_rows, up_cols, preferred_element_type=jnp.float32)
        hidden_back = lax.dot_general(slot_cot, down_rows_w, (((1,), (1,)), ((), ())), preferred_element_type=jnp.float32)
        gate_sig = jax.nn.sigmoid(gate_pre)
        activated = gate_pre * gate_sig
        hidden = activated * up_pre
        route_sum = jnp.sum(hidden * hidden_back, axis=1)
        hidden_cot = slot_scale[:, None] * hidden_back
        up_cot = (hidden_cot * activated).astype(jnp.bfloat16)
        gate_cot = (hidden_cot * up_pre * gate_sig * (1.0 + gate_pre * (1.0 - gate_sig))).astype(jnp.bfloat16)
        weighted_hidden = (slot_scale[:, None] * hidden).astype(jnp.bfloat16)
        grad_down_e = lax.dot_general(weighted_hidden, slot_cot, (((0,), (0,)), ((), ())), preferred_element_type=jnp.float32).astype(jnp.bfloat16)
        grad_gate_e = lax.dot_general(slot_rows, gate_cot, (((0,), (0,)), ((), ())), preferred_element_type=jnp.float32).astype(jnp.bfloat16)
        grad_up_e = lax.dot_general(slot_rows, up_cot, (((0,), (0,)), ((), ())), preferred_element_type=jnp.float32).astype(jnp.bfloat16)
        gate_blocks = gate_cot.astype(jnp.float32).reshape(slot_total, N_TP, quarter)
        up_blocks = up_cot.astype(jnp.float32).reshape(slot_total, N_TP, quarter)
        gate_w_blocks = gate_cols.astype(jnp.float32).reshape(D, N_TP, quarter)
        up_w_blocks = up_cols.astype(jnp.float32).reshape(D, N_TP, quarter)
        block_part = jnp.einsum('sjf,djf->sjd', gate_blocks, gate_w_blocks, precision=lax.Precision.HIGHEST)
        block_part = block_part + jnp.einsum('sjf,djf->sjd', up_blocks, up_w_blocks, precision=lax.Precision.HIGHEST)
        block_round = lax.optimization_barrier(block_part.astype(jnp.bfloat16))
        pair_grad = jnp.sum(block_round.astype(jnp.float32), axis=1).astype(jnp.bfloat16)
        return grad_gate_e, grad_up_e, grad_down_e, pair_grad, route_sum.astype(jnp.bfloat16), picked

    grad_gate, grad_up, grad_down, pair_grad, route_part, picked = lax.map(per_expert, jnp.arange(EXPERTS, dtype=jnp.int32))
    index_all = picked.reshape(-1)
    token_acc = jnp.zeros((assigns + 1, D), jnp.float32).at[index_all].set(pair_grad.reshape(-1, D).astype(jnp.float32))
    token_grad = jnp.sum(token_acc[:assigns].reshape(TOKENS, TOPK, D), axis=1).astype(jnp.bfloat16)
    route_acc = jnp.zeros((assigns + 1,), jnp.bfloat16).at[index_all].set(route_part.reshape(-1))
    route_grad = route_acc[:assigns].reshape(TOKENS, TOPK)
    gate_rows = jnp.sum(jnp.square(grad_gate.astype(jnp.float32)), axis=2)
    up_rows = jnp.sum(jnp.square(grad_up.astype(jnp.float32)), axis=2)
    down_rows = jnp.sum(jnp.square(grad_down.astype(jnp.float32)), axis=2)
    return (token_grad, route_grad, grad_gate, grad_up, grad_down, gate_rows, up_rows, down_rows)
```

```python
import functools

import jax
import jax.numpy as jnp
from jax import lax
from jax.experimental import pallas as pl
from jax.experimental.pallas import tpu as pltpu
from jax.sharding import PartitionSpec as P

MESH = pl.DeviceIdType.MESH
BF = jnp.bfloat16
F32 = jnp.float32
I32 = jnp.int32

PLANES = 8
ROW = 16
GROUP = 32
TOK = 128
SEAT = 64
RELAY = 4 * SEAT
SLOTS = 512
BLK = 16
CH = 4
CW = 256
NN = (((1,), (0,)), ((), ()))
NT = (((1,), (1,)), ((), ()))
TN = (((0,), (0,)), ((), ()))


def mm(a, b, dims=NN, precision=None):
    return lax.dot_general(a, b, dims, precision=precision, preferred_element_type=F32)


def kernel(
    ids_ref, rw_ref, tok_hbm, cot_hbm, wg_hbm, wu_hbm, wd_hbm,
    tg_ref, rg_ref, gg_hbm, gu_hbm, gd_hbm, gr_ref, ur_ref, dr_ref,
    xc, t1, sendbuf, sendmeta, relay, zmeta, p2, pairbuf, scbuf, xs, scr,
    wgu, wdb, acc_gu, acc_hb, cot, whb, rp, rall, tt, sub_p, sub_m,
    s1p, s1m, dp, dm, s2p, s2m, ret, retr, back, backr, c01, c0, c1,
    tokbuf, rtb, srcv, srcr, ggb, gub, gdb, rnall,
    ld_s, w_s, z_s, z_r, zm_s, zm_r, y_s, y_r, ys_s, ys_r, x_s, x_r,
    r_s, r_r, s_s, s_r, b_s, b_r, br_s, br_r, zb_s, zb_r, zr_s, zr_r, n_s, n_r, g_s,
):
    ep = lax.axis_index("ep")
    t = lax.axis_index("tp")
    z = ep // ROW
    yc = ep % ROW
    sg = 1 - 2 * (z % 2)
    grp = z // 2
    base = grp * GROUP
    loc = ep % GROUP
    right = (t + 1) % 4
    left = (t + 3) % 4
    far = (t + 2) % 4

    def plane(off):
        return ((z + off + PLANES) % PLANES) * ROW + yc

    out_z = [plane(-sg), plane(2 * sg), plane(-3 * sg)]
    in_z = [plane(-sg), plane(-2 * sg), plane(-3 * sg)]

    def remote(src, dst, ssem, rsem, dev):
        return pltpu.make_async_remote_copy(
            src_ref=src, dst_ref=dst, send_sem=ssem, recv_sem=rsem,
            device_id=dev, device_id_type=MESH,
        )

    def drain(ref, sem):
        pltpu.make_async_copy(ref, ref, sem).wait()

    def peer(o):
        return (loc + o) % GROUP

    def rows16(i):
        return pl.ds(pl.multiple_of(i * BLK, BLK), BLK)

    def seat(i):
        return pl.ds(pl.multiple_of(i * SEAT, SEAT), SEAT)

    cols = pl.ds(pl.multiple_of(t * 512, 512), 512)
    ld = [
        pltpu.make_async_copy(tok_hbm.at[:, cols], xc.at[:, pl.ds(0, 512)], ld_s.at[0]),
        pltpu.make_async_copy(cot_hbm.at[:, cols], xc.at[:, pl.ds(512, 512)], ld_s.at[1]),
    ]
    wl = [
        pltpu.make_async_copy(wg_hbm, wgu.at[:, pl.ds(0, 128)], w_s.at[0]),
        pltpu.make_async_copy(wu_hbm, wgu.at[:, pl.ds(128, 128)], w_s.at[1]),
    ]
    for j in range(8):
        wl.append(pltpu.make_async_copy(wd_hbm.at[:, pl.ds(j * CW, CW)], wdb.at[j], w_s.at[2 + j]))
    for c in ld:
        c.start()
    for c in wl:
        c.start()

    barrier = pltpu.get_barrier_semaphore()

    def hello(e, k):
        pl.semaphore_signal(barrier, inc=1, device_id=(e, k), device_id_type=MESH)

    for k in (right, left, far):
        hello(ep, k)
    for e in (plane(-sg), plane(2), plane(-2), plane(-3 * sg)):
        hello(e, t)

    def hello_group(o, carry):
        hello(base + peer(o), t)
        return carry

    lax.fori_loop(1, GROUP, hello_group, 0)

    ids = ids_ref[...]
    id0, id1 = ids[0:1, :], ids[1:2, :]
    sub = lax.broadcasted_iota(I32, (TOK, TOK), 0)
    lane = lax.broadcasted_iota(I32, (TOK, TOK), 1)
    oh0 = jnp.where(sub == id0, 1.0, 0.0)
    oh1 = jnp.where(sub == id1, 1.0, 0.0)
    upper = jnp.where(sub < lane, 1.0, 0.0).astype(BF)
    before = mm((oh0 + oh1).astype(BF), upper)
    k0 = jnp.sum(before * oh0, axis=0, keepdims=True)
    k1 = jnp.sum(before * oh1, axis=0, keepdims=True)
    g = id0 // GROUP
    ohg = jnp.where(lax.broadcasted_iota(I32, (16, TOK), 0) == g, 1.0, 0.0)
    q = jnp.sum(mm(ohg.astype(BF), upper) * ohg, axis=0, keepdims=True)
    slot = g * SEAT + q.astype(I32)
    code0 = ((id0 - g * GROUP) * 4).astype(F32) + k0
    code1 = ((id1 - g * GROUP) * 4).astype(F32) + k1
    rw = rw_ref[...].astype(F32)
    mrow = jnp.where(
        sub == 0, code0,
        jnp.where(sub == 1, code1, jnp.where(sub == 2, rw[0:1, :], jnp.where(sub == 3, rw[1:2, :], 0.0))),
    ).astype(BF)
    t1[...] = jnp.where(lax.broadcasted_iota(I32, (RELAY, TOK), 0) == slot, 1.0, 0.0).astype(BF)
    sendmeta[...] = mm(t1[...], mrow, NT).astype(BF)
    for c in ld:
        c.wait()
    for h in range(CH):
        sendbuf[h] = mm(t1[...], xc[:, h * CW : (h + 1) * CW]).astype(BF)

    pl.semaphore_wait(barrier, 3 + 4 + GROUP - 1)

    for d in (1, 2, 3):
        dst = out_z[d - 1]
        seats = seat(dst // GROUP)
        here = pl.ds(d * SEAT, SEAT)
        remote(sendmeta.at[seats], zmeta.at[here], zm_s, zm_r, (dst, t)).start()
    for h in range(CH):
        for d in (1, 2, 3):
            dst = out_z[d - 1]
            seats = seat(dst // GROUP)
            here = pl.ds(d * SEAT, SEAT)
            remote(sendbuf.at[h, seats], relay.at[h, here], z_s.at[h], z_r.at[h], (dst, t)).start()
    zmeta[0:SEAT, :] = sendmeta[seat(grp), :]
    for h in range(CH):
        relay[h, 0:SEAT, :] = sendbuf[h, seat(grp), :]

    for c in wl:
        c.wait()

    drain(zmeta.at[pl.ds(SEAT, 3 * SEAT)], zm_r)
    pick = jnp.where(
        lax.broadcasted_iota(I32, (16, 128), 0) == lax.broadcasted_iota(I32, (16, 128), 1), 1.0, 0.0
    ).astype(BF)
    flat = mm(pick, zmeta[...], NT)
    seatrow = lax.broadcasted_iota(I32, (1, RELAY), 1) // SEAT

    def place(code, where_seat):
        code = code.astype(I32)
        return (code // 4) * BLK + where_seat * 4 + code % 4

    pos0 = place(flat[0:1, :], seatrow)
    pos1 = place(flat[1:2, :], seatrow)
    w0, w1 = flat[2:3, :], flat[3:4, :]
    ones256 = jnp.ones((RELAY, 128), BF)

    def spread(i, carry):
        at = pl.ds(pl.multiple_of(i * 128, 128), 128)
        p = lax.broadcasted_iota(I32, (128, RELAY), 0) + i * 128
        e0, e1 = p == pos0, p == pos1
        p2[at, :] = jnp.where(e0, 1.0, jnp.where(e1, 1.0, 0.0)).astype(BF)
        weights = (jnp.where(e0, w0, 0.0) + jnp.where(e1, w1, 0.0)).astype(BF)
        scbuf[at, :] = mm(weights, ones256).astype(BF)
        return carry

    lax.fori_loop(0, 4, spread, 0)

    def send_group(src, dst, ssem, rsem):
        def body(o, carry):
            e = peer(o)
            remote(src.at[rows16(e)], dst.at[rows16(loc)], ssem, rsem, (base + e, t)).start()
            return carry

        lax.fori_loop(1, GROUP, body, 0)

    mine = rows16(loc)
    most = pl.ds(0, (GROUP - 1) * BLK)

    def relay_step(h):
        drain(relay.at[h, pl.ds(SEAT, 3 * SEAT)], z_r.at[h])
        pairbuf[h] = mm(p2[...], relay[h]).astype(BF)
        send_group(pairbuf.at[h], xs.at[t, h], y_s.at[h], y_r.at[h])
        xs[t, h, mine, :] = pairbuf[h, mine, :]

    half0, half1 = pl.ds(0, 256), pl.ds(256, 256)

    def x_copies(h):
        return (
            remote(xs.at[t, h], xs.at[t, h], x_s.at[h, 0], x_r.at[h, 0], (ep, right)),
            remote(xs.at[t, h], xs.at[t, h], x_s.at[h, 1], x_r.at[h, 1], (ep, left)),
        )

    def f_copies(h):
        return (
            remote(xs.at[left, h, half0], xs.at[left, h, half0], x_s.at[h, 2], x_r.at[h, 2], (ep, right)),
            remote(xs.at[right, h, half1], xs.at[right, h, half1], x_s.at[h, 3], x_r.at[h, 3], (ep, left)),
        )

    def gather_step(h):
        drain(pairbuf.at[h, most], y_r.at[h])
        for c in x_copies(h):
            c.start()

    def forward_step(h):
        for c in x_copies(h):
            c.wait_recv()
        for c in f_copies(h):
            c.start()

    def arrive_step(h):
        for c in f_copies(h):
            c.wait_recv()

    def product(k, h, first=False):
        if h < 2:
            at = pl.ds(pl.multiple_of(k * 512 + h * CW, CW), CW)
            part = mm(xs[k, h], wgu[at, :])
            if first:
                acc_gu[...] = part
            else:
                acc_gu[...] += part
        else:
            part = mm(xs[k, h], wdb[k * 2 + (h - 2)], NT)
            if first:
                acc_hb[...] = part
            else:
                acc_hb[...] += part

    def near_products(h):
        product(t, h, first=(h % 2 == 0))

        def body(i, carry):
            product((t + 1 + 2 * i) % 4, h)
            return carry

        lax.fori_loop(0, 2, body, 0)

    relay_step(0)
    send_group(scbuf, scr, ys_s, ys_r)
    scr[mine, :] = scbuf[mine, :]
    relay_step(1)
    relay_step(2)
    gather_step(0)
    relay_step(3)
    gather_step(1)
    forward_step(0)
    near_products(0)

    seatcol = lax.broadcasted_iota(I32, (RELAY, 1), 0) // SEAT
    codes = zmeta[...].astype(F32)
    back0 = place(codes[:, 0:1], seatcol)
    back1 = place(codes[:, 1:2], seatcol)
    wide = lax.broadcasted_iota(I32, (RELAY, SLOTS), 1)
    m0 = jnp.where(wide == back0, 1.0, 0.0)
    m1 = jnp.where(wide == back1, 1.0, 0.0)
    c0[...] = m0.astype(BF)
    c1[...] = m1.astype(BF)
    c01[...] = (m0 + m1).astype(BF)

    gather_step(2)
    forward_step(1)
    near_products(1)
    gather_step(3)
    forward_step(2)
    near_products(2)
    arrive_step(0)
    product(far, 0)
    arrive_step(1)
    product(far, 1)
    forward_step(3)
    near_products(3)
    arrive_step(2)
    product(far, 2)
    drain(scbuf.at[most], ys_r)
    arrive_step(3)
    product(far, 3)

    def activate(i, carry):
        at = pl.ds(pl.multiple_of(i * 64, 64), 64)
        gate, up = acc_gu[at, 0:128], acc_gu[at, 128:256]
        hb = acc_hb[at, :]
        sc = scr[at, :].astype(F32)
        sig = jax.nn.sigmoid(gate)
        act = gate * sig
        hid = act * up
        hc = sc * hb
        cot[at, 0:128] = (hc * up * sig * (1.0 + gate * (1.0 - sig))).astype(BF)
        cot[at, 128:256] = (hc * act).astype(BF)
        whb[at, :] = (sc * hid).astype(BF)
        rp[at, :] = hid * hb
        return carry

    lax.fori_loop(0, 8, activate, 0)

    def share(k, p):
        at = pl.ds(pl.multiple_of(k * 512 + p * CW, CW), CW)
        part = mm(cot[...], wgu[at, :], NT).astype(BF)
        tt[k, 2 * p] = part[:, 0:128]
        tt[k, 2 * p + 1] = part[:, 128:256]

    def s1_copies(p):
        return (
            remote(tt.at[far, 2 * p], s1p.at[p], s_s.at[p, 0], s_r.at[p, 0], (ep, right)),
            remote(tt.at[far, 2 * p + 1], s1m.at[p], s_s.at[p, 1], s_r.at[p, 1], (ep, left)),
        )

    def d_copies(p):
        return (
            remote(tt.at[right, 2 * p + 1], dp.at[p], s_s.at[p, 2], s_r.at[p, 2], (ep, right)),
            remote(tt.at[left, 2 * p], dm.at[p], s_s.at[p, 3], s_r.at[p, 3], (ep, left)),
        )

    def s2_copies(p):
        return (
            remote(sub_p.at[p], s2p.at[p], s_s.at[p, 4], s_r.at[p, 4], (ep, right)),
            remote(sub_m.at[p], s2m.at[p], s_s.at[p, 5], s_r.at[p, 5], (ep, left)),
        )

    def everyone(buf, ssem, rsem):
        return [
            remote(buf.at[t], buf.at[t], ssem.at[i], rsem.at[i], (ep, k))
            for i, k in enumerate((right, left, far))
        ]

    share(far, 0)
    for c in s1_copies(0):
        c.start()
    share(right, 0)
    share(left, 0)
    for c in d_copies(0):
        c.start()

    ones16 = jnp.ones((16, 128), F32)
    rsum = mm(ones16, rp[...], NT, lax.Precision.HIGHEST)
    rall[t] = rsum[0:8, :]
    share(far, 1)
    share(right, 1)
    share(left, 1)
    r_copies = everyone(rall, r_s, r_r)
    for c in r_copies:
        c.start()
    share(t, 0)
    share(t, 1)

    def second(p):
        for c in s1_copies(p):
            c.wait_recv()
        sub_p[p] = (s1p[p].astype(F32) + tt[right, 2 * p].astype(F32)).astype(BF)
        sub_m[p] = (s1m[p].astype(F32) + tt[left, 2 * p + 1].astype(F32)).astype(BF)
        for c in s2_copies(p):
            c.start()

    def reduced(p):
        for c in (*s2_copies(p), *d_copies(p)):
            c.wait_recv()
        ret[p, :, 0:128] = (
            tt[t, 2 * p].astype(F32) + s2p[p].astype(F32) + dm[p].astype(F32)
        ).astype(BF)
        ret[p, :, 128:256] = (
            tt[t, 2 * p + 1].astype(F32) + s2m[p].astype(F32) + dp[p].astype(F32)
        ).astype(BF)
        send_group(ret.at[p], back.at[p], b_s.at[p], b_r.at[p])
        back[p, mine, :] = ret[p, mine, :]

    ones8 = jnp.ones((16, 128), F32)

    def wgrad(j):
        k, h = j // 2, j % 2
        d0 = pl.multiple_of(j * CW, CW)
        at = pl.ds(d0, CW)
        both = mm(xs[k, h], cot[...], TN).astype(BF)
        ggb[at, :] = both[:, 0:128]
        gub[at, :] = both[:, 128:256]
        sq = jnp.square(both.astype(F32))
        ng = mm(ones8, sq[:, 0:128], NT, lax.Precision.HIGHEST)
        nu = mm(ones8, sq[:, 128:256], NT, lax.Precision.HIGHEST)
        rnall[t, pl.ds(2 * j, 1), :] = ng[0:1, 0:128]
        rnall[t, pl.ds(2 * j + 1, 1), :] = ng[0:1, 128:256]
        rnall[t, pl.ds(16 + 2 * j, 1), :] = nu[0:1, 0:128]
        rnall[t, pl.ds(17 + 2 * j, 1), :] = nu[0:1, 128:256]

    def dgrad(j, total):
        k, h = j // 2, j % 2
        down = mm(whb[...], xs[k, 2 + h], TN).astype(BF)
        gdb[j] = down
        sq = jnp.square(down.astype(F32))
        return total + sq[:, 0:128] + sq[:, 128:256]

    def wgrads(lo, hi):
        def body(j, carry):
            wgrad(j)
            return carry

        lax.fori_loop(lo, hi, body, 0)

    wgrads(0, 4)
    second(0)
    for c in s1_copies(1):
        c.start()
    for c in d_copies(1):
        c.start()
    wgrads(4, 8)
    n_copies = everyone(rnall, n_s, n_r)
    for c in n_copies:
        c.start()
    gcopies = [
        pltpu.make_async_copy(ggb, gg_hbm, g_s.at[0]),
        pltpu.make_async_copy(gub, gu_hbm, g_s.at[1]),
    ]
    for c in gcopies:
        c.start()

    for c in r_copies:
        c.wait_recv()
    rtot = ((rall[0] + rall[1]) + rall[2]) + rall[3]
    rtot = jnp.where(lax.broadcasted_iota(I32, (8, SLOTS), 0) == 0, rtot, 0.0)
    retr[...] = mm(rtot.astype(BF), jnp.ones((8, 128), BF), TN).astype(BF)
    reduced(0)
    send_group(retr, backr, br_s, br_r)
    backr[mine, :] = retr[mine, :]
    second(1)

    total = lax.fori_loop(0, 8, dgrad, jnp.zeros((128, 128), F32))
    dcopies = [
        pltpu.make_async_copy(gdb.at[j], gd_hbm.at[:, pl.ds(j * CW, CW)], g_s.at[2 + j])
        for j in range(8)
    ]
    for c in dcopies:
        c.start()
    dr_ref[...] = mm(ones16, total, NT, lax.Precision.HIGHEST)[0:1, :]

    def home(src, dst, ssem, rsem):
        for d in (1, 2, 3):
            remote(src.at[pl.ds(d * SEAT, SEAT)], dst.at[seat(grp)], ssem, rsem, (in_z[d - 1], t)).start()

    def combine(p):
        drain(ret.at[p, most], b_r.at[p])
        tokbuf[p] = mm(c01[...], back[p]).astype(BF)
        home(tokbuf.at[p], srcv.at[p], zb_s.at[p], zb_r.at[p])
        srcv[p, seat(grp), :] = tokbuf[p, 0:SEAT, :]

    reduced(1)
    combine(0)
    drain(retr.at[most], br_r)
    lane2 = lax.broadcasted_iota(I32, (RELAY, 128), 1)
    rtb[...] = jnp.where(lane2 == 0, mm(c0[...], backr[...]), mm(c1[...], backr[...])).astype(BF)
    home(rtb, srcr, zr_s, zr_r)
    srcr[seat(grp), :] = rtb[0:SEAT, :]

    for c in n_copies:
        c.wait_recv()
    norms = ((rnall[0] + rnall[1]) + rnall[2]) + rnall[3]
    gr_ref[...] = norms[0:16, :]
    ur_ref[...] = norms[16:32, :]
    combine(1)

    three = pl.ds(0, 3 * SEAT)
    drain(tokbuf.at[0, three], zb_r.at[0])
    tg_ref[:, 0:256] = mm(t1[...], srcv[0], TN).astype(BF)
    drain(rtb.at[three], zr_r)
    rg_ref[...] = mm(srcr[...], t1[...], TN)[0:2, :].astype(BF)

    drain(sendmeta.at[three], zm_s)
    for h in range(CH):
        drain(sendbuf.at[h, three], z_s.at[h])
        drain(pairbuf.at[h, most], y_s.at[h])
        for c in (*x_copies(h), *f_copies(h)):
            c.wait_send()
    drain(scbuf.at[most], ys_s)
    for c in (*r_copies, *n_copies):
        c.wait_send()
    for p in range(2):
        for c in (*s1_copies(p), *d_copies(p), *s2_copies(p)):
            c.wait_send()
        drain(ret.at[p, most], b_s.at[p])
        drain(tokbuf.at[p, three], zb_s.at[p])
    drain(retr.at[most], br_s)
    drain(rtb.at[three], zr_s)
    for c in (*gcopies, *dcopies):
        c.wait()
    drain(tokbuf.at[1, three], zb_r.at[1])
    tg_ref[:, 256:512] = mm(t1[...], srcv[1], TN).astype(BF)


def on_device(tokens, expert_ids, route_weights, cotangent, w_gate, w_up, w_down):
    vmem = pl.BlockSpec(memory_space=pltpu.VMEM)
    hbm = pl.BlockSpec(memory_space=pl.ANY)
    dma = pltpu.SemaphoreType.DMA
    v = pltpu.VMEM
    scratch = [
        v((TOK, 1024), BF),
        v((RELAY, TOK), BF),
        v((CH, RELAY, CW), BF),
        v((RELAY, 128), BF),
        v((CH, RELAY, CW), BF),
        v((RELAY, 128), BF),
        v((SLOTS, RELAY), BF),
        v((CH, SLOTS, CW), BF),
        v((SLOTS, 128), BF),
        v((4, CH, SLOTS, CW), BF),
        v((SLOTS, 128), BF),
        v((2048, 256), BF),
        v((8, 128, CW), BF),
        v((SLOTS, 256), F32),
        v((SLOTS, 128), F32),
        v((SLOTS, 256), BF),
        v((SLOTS, 128), BF),
        v((SLOTS, 128), F32),
        v((4, 8, SLOTS), F32),
        v((4, 4, SLOTS, 128), BF),
        v((2, SLOTS, 128), BF),
        v((2, SLOTS, 128), BF),
        v((2, SLOTS, 128), BF),
        v((2, SLOTS, 128), BF),
        v((2, SLOTS, 128), BF),
        v((2, SLOTS, 128), BF),
        v((2, SLOTS, 128), BF),
        v((2, SLOTS, 128), BF),
        v((2, SLOTS, CW), BF),
        v((SLOTS, 128), BF),
        v((2, SLOTS, CW), BF),
        v((SLOTS, 128), BF),
        v((RELAY, SLOTS), BF),
        v((RELAY, SLOTS), BF),
        v((RELAY, SLOTS), BF),
        v((2, RELAY, CW), BF),
        v((RELAY, 128), BF),
        v((2, RELAY, CW), BF),
        v((RELAY, 128), BF),
        v((2048, 128), BF),
        v((2048, 128), BF),
        v((8, 128, CW), BF),
        v((4, 32, 128), F32),
        dma((2,)), dma((10,)),
        dma((CH,)), dma((CH,)), dma(()), dma(()),
        dma((CH,)), dma((CH,)), dma(()), dma(()),
        dma((CH, 4)), dma((CH, 4)),
        dma((3,)), dma((3,)),
        dma((2, 6)), dma((2, 6)),
        dma((2,)), dma((2,)), dma(()), dma(()),
        dma((2,)), dma((2,)), dma(()), dma(()),
        dma((3,)), dma((3,)), dma((10,)),
    ]
    s = jax.ShapeDtypeStruct
    tg, rg, gg, gu, gd, gr, ur, dr = pl.pallas_call(
        kernel,
        out_shape=(
            s((TOK, 512), BF), s((2, TOK), BF), s((2048, 128), BF), s((2048, 128), BF),
            s((128, 2048), BF), s((16, 128), F32), s((16, 128), F32), s((1, 128), F32),
        ),
        in_specs=[vmem, vmem, hbm, hbm, hbm, hbm, hbm],
        out_specs=(vmem, vmem, hbm, hbm, hbm, vmem, vmem, vmem),
        scratch_shapes=scratch,
        compiler_params=pltpu.CompilerParams(collective_id=0, has_side_effects=True),
    )(expert_ids.T, route_weights.T, tokens, cotangent, w_gate[0], w_up[0], w_down[0])
    return (
        tg, rg.T, gg[None], gu[None], gd[None],
        gr.reshape(1, 2048), ur.reshape(1, 2048), dr,
    )


def solution(mesh):
    return jax.shard_map(
        on_device,
        mesh=mesh,
        in_specs=(
            P("ep", None), P("ep", None), P("ep", None), P("ep", None),
            P("ep", None, "tp"), P("ep", None, "tp"), P("ep", "tp", None),
        ),
        out_specs=(
            P("ep", "tp"), P("ep", None), P("ep", None, "tp"), P("ep", None, "tp"),
            P("ep", "tp", None), P("ep", None), P("ep", None), P("ep", "tp"),
        ),
        check_vma=False,
    )
```

```python
import functools

import jax
import jax.numpy as jnp
from jax import lax
from jax.experimental import pallas as pl
from jax.experimental.pallas import tpu as pltpu
from jax.sharding import PartitionSpec as P

MESH = pl.DeviceIdType.MESH
BF = jnp.bfloat16
F32 = jnp.float32
I32 = jnp.int32

PLANES = 8
ROW = 16
GROUP = 32
TOK = 128
SEAT = 64
RELAY = 4 * SEAT
SLOTS = 512
BLK = 16
CHUNKS = ((0, 1), (1, 1), (2, 1), (3, 1), (4, 2), (6, 2))
NN = (((1,), (0,)), ((), ()))
NT = (((1,), (1,)), ((), ()))
TN = (((0,), (0,)), ((), ()))


def mm(a, b, dims=NN, precision=None):
    return lax.dot_general(a, b, dims, precision=precision, preferred_element_type=F32)


def kernel(
    ids_hbm, rw_hbm, tok_hbm, cot_hbm, wg_hbm, wu_hbm, wd_hbm,
    tg_ref, rg_ref, ggb, gub, gdr, gr_ref, ur_ref, dr_ref,
    xc, t1, sendbuf, sendmeta, relay, zmeta, p2, pairbuf, scbuf, xs, cs, scr,
    wgu, wdd, acc_gu, acc_hb, cot, wha, rp, rall, tt, sub_p, sub_m,
    s1p, s1m, dp, dm, s2p, s2m, ret, retr, back, backr, c01, c0, c1,
    tokbuf, rtb, srcv, srcr, gds, gdin, rnall, ids_v, rw_v,
    ld_s, w_s, z_s, z_r, zm_s, zm_r, y_s, y_r, ys_s, ys_r, x_s, x_r, h_s, h_r, v_s, v_r, e_s, e_r,
    r_s, r_r, s_s, s_r, b_s, b_r, br_s, br_r, zb_s, zb_r, zr_s, zr_r, n_s, n_r,
):
    ep = lax.axis_index("ep")
    t = lax.axis_index("tp")
    z = ep // ROW
    yc = ep % ROW
    sg = 1 - 2 * (z % 2)
    grp = z // 2
    base = grp * GROUP
    loc = ep % GROUP
    right = (t + 1) % 4
    left = (t + 3) % 4
    far = (t + 2) % 4

    def plane(off):
        return ((z + off + PLANES) % PLANES) * ROW + yc

    out_z = [plane(-sg), plane(2 * sg), plane(-3 * sg)]
    in_z = [plane(-sg), plane(-2 * sg), plane(-3 * sg)]

    def remote(src, dst, ssem, rsem, dev):
        return pltpu.make_async_remote_copy(
            src_ref=src, dst_ref=dst, send_sem=ssem, recv_sem=rsem,
            device_id=dev, device_id_type=MESH,
        )

    def drain(ref, sem):
        pltpu.make_async_copy(ref, ref, sem).wait()

    def begin(copies):
        for c in copies:
            c.start()

    def landed(copies):
        for c in copies:
            c.wait_recv()

    def left_here(copies):
        for c in copies:
            c.wait_send()

    def peer(o):
        return (loc + o) % GROUP

    def rows16(i):
        return pl.ds(pl.multiple_of(i * BLK, BLK), BLK)

    def seat(i):
        return pl.ds(pl.multiple_of(i * SEAT, SEAT), SEAT)

    def block(k):
        return pl.ds(pl.multiple_of(k * 512, 512), 512)

    route_in = [
        pltpu.make_async_copy(ids_hbm, ids_v, ld_s.at[2]),
        pltpu.make_async_copy(rw_hbm, rw_v, ld_s.at[3]),
    ]
    begin(route_in)
    ld = [
        pltpu.make_async_copy(tok_hbm.at[:, block(t)], xc.at[:, pl.ds(0, 512)], ld_s.at[0]),
        pltpu.make_async_copy(cot_hbm.at[:, block(t)], xc.at[:, pl.ds(512, 512)], ld_s.at[1]),
    ]
    wl = [
        pltpu.make_async_copy(wg_hbm, wgu.at[:, pl.ds(0, 128)], w_s.at[0]),
        pltpu.make_async_copy(wu_hbm, wgu.at[:, pl.ds(128, 128)], w_s.at[1]),
        pltpu.make_async_copy(wd_hbm.at[:, block(t)], wdd.at[t], w_s.at[2]),
    ]
    begin(ld)

    barrier = pltpu.get_barrier_semaphore()

    def hello(e, k):
        pl.semaphore_signal(barrier, inc=1, device_id=(e, k), device_id_type=MESH)

    for e in (plane(-3 * sg), plane(2), plane(-2), plane(-sg)):
        hello(e, t)
    for k in (far, right, left):
        hello(ep, k)

    def hello_group(o, carry):
        hello(base + peer(o), t)
        return carry

    lax.fori_loop(1, GROUP, hello_group, 0)

    for c in route_in:
        c.wait()
    ids = ids_v[...]
    id0, id1 = ids[0:1, :], ids[1:2, :]
    sub = lax.broadcasted_iota(I32, (TOK, TOK), 0)
    lane = lax.broadcasted_iota(I32, (TOK, TOK), 1)
    oh0 = jnp.where(sub == id0, 1.0, 0.0)
    oh1 = jnp.where(sub == id1, 1.0, 0.0)
    upper = jnp.where(sub < lane, 1.0, 0.0).astype(BF)
    before = mm((oh0 + oh1).astype(BF), upper)
    k0 = jnp.sum(before * oh0, axis=0, keepdims=True)
    k1 = jnp.sum(before * oh1, axis=0, keepdims=True)
    g = id0 // GROUP
    ohg = jnp.where(lax.broadcasted_iota(I32, (16, TOK), 0) == g, 1.0, 0.0)
    q = jnp.sum(mm(ohg.astype(BF), upper) * ohg, axis=0, keepdims=True)
    slot = g * SEAT + q.astype(I32)
    code0 = ((id0 - g * GROUP) * 4).astype(F32) + k0
    code1 = ((id1 - g * GROUP) * 4).astype(F32) + k1
    rw = rw_v[...].astype(F32)
    mrow = jnp.where(
        sub == 0, code0,
        jnp.where(sub == 1, code1, jnp.where(sub == 2, rw[0:1, :], jnp.where(sub == 3, rw[1:2, :], 0.0))),
    ).astype(BF)
    t1[...] = jnp.where(lax.broadcasted_iota(I32, (RELAY, TOK), 0) == slot, 1.0, 0.0).astype(BF)
    sendmeta[...] = mm(t1[...], mrow, NT).astype(BF)
    for c in ld:
        c.wait()
    for h in range(4):
        part = mm(t1[...], xc[:, h * 256 : (h + 1) * 256]).astype(BF)
        sendbuf[2 * h] = part[:, 0:128]
        sendbuf[2 * h + 1] = part[:, 128:256]

    pl.semaphore_wait(barrier, 3 + 4 + GROUP - 1)

    def send_meta():
        for d in (1, 2, 3):
            dst = out_z[d - 1]
            here = pl.ds(d * SEAT, SEAT)
            remote(sendmeta.at[seat(dst // GROUP)], zmeta.at[here], zm_s, zm_r, (dst, t)).start()

    def send_z(i):
        qs = pl.ds(*CHUNKS[i])
        for d in (1, 2, 3):
            dst = out_z[d - 1]
            here = pl.ds(d * SEAT, SEAT)
            remote(
                sendbuf.at[qs, seat(dst // GROUP)], relay.at[qs, here], z_s.at[i], z_r.at[i], (dst, t)
            ).start()

    exch = [
        remote(wd_hbm.at[:, block(k)], wdd.at[t], e_s.at[i], e_r.at[i], (ep, k))
        for i, k in enumerate((right, left, far))
    ]
    send_meta()
    send_z(0)
    send_z(1)
    begin(wl)
    begin(exch)
    zmeta[0:SEAT, :] = sendmeta[seat(grp), :]
    for h in range(8):
        relay[h, 0:SEAT, :] = sendbuf[h, seat(grp), :]

    drain(zmeta.at[pl.ds(SEAT, 3 * SEAT)], zm_r)
    send_z(2)
    pick = jnp.where(
        lax.broadcasted_iota(I32, (16, 128), 0) == lax.broadcasted_iota(I32, (16, 128), 1), 1.0, 0.0
    ).astype(BF)
    flat = mm(pick, zmeta[...], NT)
    seatrow = lax.broadcasted_iota(I32, (1, RELAY), 1) // SEAT

    def place(code, where_seat):
        code = code.astype(I32)
        return (code // 4) * BLK + where_seat * 4 + code % 4

    pos0 = place(flat[0:1, :], seatrow)
    pos1 = place(flat[1:2, :], seatrow)
    w0, w1 = flat[2:3, :], flat[3:4, :]
    ones256 = jnp.ones((RELAY, 128), BF)

    def spread(i, carry):
        at = pl.ds(pl.multiple_of(i * 128, 128), 128)
        p = lax.broadcasted_iota(I32, (128, RELAY), 0) + i * 128
        e0, e1 = p == pos0, p == pos1
        p2[at, :] = jnp.where(e0, 1.0, jnp.where(e1, 1.0, 0.0)).astype(BF)
        weights = (jnp.where(e0, w0, 0.0) + jnp.where(e1, w1, 0.0)).astype(BF)
        scbuf[at, :] = mm(weights, ones256).astype(BF)
        return carry

    lax.fori_loop(0, 4, spread, 0)

    def send_group(src, dst, ssem, rsem):
        def body(o, carry):
            e = peer(o)
            remote(src(rows16(e)), dst(rows16(loc)), ssem, rsem, (base + e, t)).start()
            return carry

        lax.fori_loop(1, GROUP, body, 0)

    mine = rows16(loc)
    most = pl.ds(0, (GROUP - 1) * BLK)

    def relay_step(i):
        q0, n = CHUNKS[i]
        drain(relay.at[pl.ds(q0, n), pl.ds(SEAT, 3 * SEAT)], z_r.at[i])
        rows = relay[q0] if n == 1 else jnp.concatenate([relay[q0], relay[q0 + 1]], axis=1)
        out = mm(p2[...], rows).astype(BF)
        for k in range(n):
            pairbuf[q0 + k] = out[:, k * 128 : (k + 1) * 128]
        qs = pl.ds(q0, n)
        if q0 < 4:
            send_group(
                lambda r: pairbuf.at[qs, r], lambda r: xs.at[t, qs, r], y_s.at[i], y_r.at[i]
            )
            for k in range(n):
                xs[t, q0 + k, mine, :] = pairbuf[q0 + k, mine, :]
        else:
            qc = pl.ds(q0 - 4, n)
            send_group(
                lambda r: pairbuf.at[qs, r], lambda r: cs.at[qc, r], y_s.at[i], y_r.at[i]
            )
            for k in range(n):
                cs[q0 - 4 + k, mine, :] = pairbuf[q0 + k, mine, :]

    def routed(i):
        drain(pairbuf.at[pl.ds(*CHUNKS[i]), most], y_r.at[i])

    half0, half1 = pl.ds(0, 256), pl.ds(256, 256)

    def x_copies(i):
        qs = pl.ds(*CHUNKS[i])
        return (
            remote(xs.at[t, qs], xs.at[t, qs], x_s.at[i, 0], x_r.at[i, 0], (ep, right)),
            remote(xs.at[t, qs], xs.at[t, qs], x_s.at[i, 1], x_r.at[i, 1], (ep, left)),
        )

    def f_copies(i):
        qs = pl.ds(*CHUNKS[i])
        return (
            remote(xs.at[left, qs, half0], xs.at[left, qs, half0], x_s.at[i, 2], x_r.at[i, 2], (ep, right)),
            remote(xs.at[right, qs, half1], xs.at[right, qs, half1], x_s.at[i, 3], x_r.at[i, 3], (ep, left)),
        )

    def forward_step(i):
        landed(x_copies(i))
        begin(f_copies(i))

    def product(k, i, first=False):
        q0, n = CHUNKS[i]
        at = pl.ds(pl.multiple_of(k * 512 + q0 * 128, 128), n * 128)
        rows = xs[k, q0] if n == 1 else jnp.concatenate([xs[k, q0], xs[k, q0 + 1]], axis=1)
        part = mm(rows, wgu[at, :])
        if first:
            acc_gu[...] = part
        else:
            acc_gu[...] += part

    def near_products(i):
        def body(j, carry):
            product((t + 1 + 2 * j) % 4, i)
            return carry

        lax.fori_loop(0, 2, body, 0)

    def hb_part(c, first):
        rows = jnp.concatenate([cs[2 * c], cs[2 * c + 1]], axis=1)

        def body(k, carry):
            part = mm(rows, wdd[k, :, c * 256 : (c + 1) * 256], NT)
            if first:
                acc_hb[k] = part
            else:
                tt[k, 4] = (acc_hb[k] + part).astype(BF)
            return carry

        lax.fori_loop(0, 4, body, 0)

    def s1_copies(p):
        return (
            remote(tt.at[far, p, half0], s1p.at[p], s_s.at[p, 0], s_r.at[p, 0], (ep, right)),
            remote(tt.at[far, p, half1], s1m.at[p], s_s.at[p, 1], s_r.at[p, 1], (ep, left)),
        )

    def d_copies(p):
        return (
            remote(tt.at[right, p, half1], dp.at[p], s_s.at[p, 2], s_r.at[p, 2], (ep, right)),
            remote(tt.at[left, p, half0], dm.at[p], s_s.at[p, 3], s_r.at[p, 3], (ep, left)),
        )

    def s2_copies(p):
        return (
            remote(sub_p.at[p], s2p.at[p], s_s.at[p, 4], s_r.at[p, 4], (ep, right)),
            remote(sub_m.at[p], s2m.at[p], s_s.at[p, 5], s_r.at[p, 5], (ep, left)),
        )

    def second(p):
        landed(s1_copies(p))
        sub_p[p] = (s1p[p].astype(F32) + tt[right, p, 0:256, :].astype(F32)).astype(BF)
        sub_m[p] = (s1m[p].astype(F32) + tt[left, p, 256:512, :].astype(F32)).astype(BF)
        begin(s2_copies(p))

    def total_of(p):
        landed(s2_copies(p))
        landed(d_copies(p))
        top = tt[t, p, 0:256, :].astype(F32) + s2p[p].astype(F32) + dm[p].astype(F32)
        low = tt[t, p, 256:512, :].astype(F32) + s2m[p].astype(F32) + dp[p].astype(F32)
        return top, low

    relay_step(0)
    relay_step(1)
    send_z(3)
    send_z(4)
    for c in wl:
        c.wait()
    routed(0)
    begin(x_copies(0))
    product(t, 0, first=True)
    relay_step(2)
    send_z(5)
    routed(1)
    begin(x_copies(1))
    product(t, 1)
    relay_step(3)
    forward_step(0)
    near_products(0)
    routed(2)
    begin(x_copies(2))
    product(t, 2)
    relay_step(4)
    forward_step(1)
    near_products(1)
    routed(3)
    begin(x_copies(3))
    product(t, 3)
    landed(f_copies(0))
    product(far, 0)

    seatcol = lax.broadcasted_iota(I32, (RELAY, 1), 0) // SEAT
    codes = zmeta[...].astype(F32)
    back0 = place(codes[:, 0:1], seatcol)
    back1 = place(codes[:, 1:2], seatcol)
    wide = lax.broadcasted_iota(I32, (RELAY, SLOTS), 1)
    m0 = jnp.where(wide == back0, 1.0, 0.0)
    m1 = jnp.where(wide == back1, 1.0, 0.0)
    c0[...] = m0.astype(BF)
    c1[...] = m1.astype(BF)
    c01[...] = (m0 + m1).astype(BF)

    relay_step(5)
    send_group(lambda r: scbuf.at[r], lambda r: scr.at[r], ys_s, ys_r)
    scr[mine, :] = scbuf[mine, :]
    landed(exch)
    forward_step(2)
    near_products(2)
    landed(f_copies(1))
    product(far, 1)
    routed(4)
    hb_part(0, True)
    forward_step(3)
    near_products(3)
    routed(5)
    hb_part(1, False)
    begin(s1_copies(4))
    begin(d_copies(4))
    landed(f_copies(2))
    product(far, 2)
    landed(f_copies(3))
    product(far, 3)

    drain(scbuf.at[most], ys_r)

    def hiddens(i, carry):
        at = pl.ds(pl.multiple_of(i * 64, 64), 64)
        gate, up = acc_gu[at, 0:128], acc_gu[at, 128:256]
        hid = gate * jax.nn.sigmoid(gate) * up
        wha[t, at, :] = (scr[at, :].astype(F32) * hid).astype(BF)
        return carry

    lax.fori_loop(0, 8, hiddens, 0)
    h_near = (
        remote(wha.at[t], wha.at[t], h_s.at[0], h_r.at[0], (ep, right)),
        remote(wha.at[t], wha.at[t], h_s.at[1], h_r.at[1], (ep, left)),
    )
    h_far = (
        remote(wha.at[left, half0], wha.at[left, half0], h_s.at[2], h_r.at[2], (ep, right)),
        remote(wha.at[right, half1], wha.at[right, half1], h_s.at[3], h_r.at[3], (ep, left)),
    )
    second(4)
    begin(h_near)
    hb_top, hb_low = total_of(4)
    acc_hb[0, 0:256, :] = hb_top
    acc_hb[0, 256:512, :] = hb_low

    def activate(i, carry):
        at = pl.ds(pl.multiple_of(i * 64, 64), 64)
        gate, up = acc_gu[at, 0:128], acc_gu[at, 128:256]
        hb = acc_hb[0, at, :]
        sc = scr[at, :].astype(F32)
        sig = jax.nn.sigmoid(gate)
        act = gate * sig
        hc = sc * hb
        cot[at, 0:128] = (hc * up * sig * (1.0 + gate * (1.0 - sig))).astype(BF)
        cot[at, 128:256] = (hc * act).astype(BF)
        rp[at, :] = act * up * hb
        return carry

    lax.fori_loop(0, 8, activate, 0)

    def share(k, p):
        at = pl.ds(pl.multiple_of(k * 512 + p * 256, 256), 256)
        part = mm(cot[...], wgu[at, :], NT).astype(BF)
        tt[k, 2 * p] = part[:, 0:128]
        tt[k, 2 * p + 1] = part[:, 128:256]

    def everyone(buf, ssem, rsem):
        return [
            remote(buf.at[t], buf.at[t], ssem.at[i], rsem.at[i], (ep, k))
            for i, k in enumerate((right, left, far))
        ]

    share(far, 0)
    begin(s1_copies(0))
    begin(s1_copies(1))
    share(right, 0)
    share(left, 0)
    begin(d_copies(0))
    ones16 = jnp.ones((16, 128), F32)
    rsum = mm(ones16, rp[...], NT, lax.Precision.HIGHEST)
    rall[t] = rsum[0:8, :]
    share(far, 1)
    share(right, 1)
    share(left, 1)
    r_copies = everyone(rall, r_s, r_r)
    begin(r_copies)
    share(t, 0)
    share(t, 1)

    def wgrad(j):
        k, h = j // 2, j % 2
        at = pl.ds(pl.multiple_of(j * 256, 256), 256)
        rows = jnp.concatenate([xs[k, 2 * h], xs[k, 2 * h + 1]], axis=1)
        both = mm(rows, cot[...], TN).astype(BF)
        ggb[at, :] = both[:, 0:128]
        gub[at, :] = both[:, 128:256]
        sq = jnp.square(both.astype(F32))
        ng = mm(ones16, sq[:, 0:128], NT, lax.Precision.HIGHEST)
        nu = mm(ones16, sq[:, 128:256], NT, lax.Precision.HIGHEST)
        rnall[t, pl.ds(2 * j, 1), :] = ng[0:1, 0:128]
        rnall[t, pl.ds(2 * j + 1, 1), :] = ng[0:1, 128:256]
        rnall[t, pl.ds(16 + 2 * j, 1), :] = nu[0:1, 0:128]
        rnall[t, pl.ds(17 + 2 * j, 1), :] = nu[0:1, 128:256]

    def wgrads(lo, hi):
        def body(j, carry):
            wgrad(j)
            return carry

        lax.fori_loop(lo, hi, body, 0)

    def reduced(p):
        top, low = total_of(p)
        ret[p, 0:256, :] = top.astype(BF)
        ret[p, 256:512, :] = low.astype(BF)
        send_group(lambda r: ret.at[p, r], lambda r: back.at[p, r], b_s.at[p], b_r.at[p])
        back[p, mine, :] = ret[p, mine, :]

    def home(src, dst, ssem, rsem):
        for d in (1, 2, 3):
            remote(src.at[pl.ds(d * SEAT, SEAT)], dst.at[seat(grp)], ssem, rsem, (in_z[d - 1], t)).start()

    def combine(p):
        drain(ret.at[p, most], b_r.at[p])
        tokbuf[p] = mm(c01[...], back[p]).astype(BF)
        home(tokbuf.at[p], srcv.at[p], zb_s.at[p], zb_r.at[p])
        srcv[p, seat(grp), :] = tokbuf[p, 0:SEAT, :]

    second(0)
    begin(d_copies(1))
    begin(s1_copies(2))
    wgrads(0, 2)
    second(1)
    begin(s1_copies(3))
    begin(d_copies(2))

    landed(r_copies)
    rtot = ((rall[0] + rall[1]) + rall[2]) + rall[3]
    rtot = jnp.where(lax.broadcasted_iota(I32, (8, SLOTS), 0) == 0, rtot, 0.0)
    retr[...] = mm(rtot.astype(BF), jnp.ones((8, 128), BF), TN).astype(BF)
    send_group(lambda r: retr.at[r], lambda r: backr.at[r], br_s, br_r)
    backr[mine, :] = retr[mine, :]

    landed(h_near)
    begin(h_far)
    reduced(0)
    second(2)
    begin(d_copies(3))
    wgrads(2, 4)
    reduced(1)
    second(3)
    wgrads(4, 6)

    landed(h_far)
    crows = [jnp.concatenate([cs[0], cs[1]], axis=1), jnp.concatenate([cs[2], cs[3]], axis=1)]

    def dgrad(k, carry):
        for c in range(2):
            gds[k, :, c * 256 : (c + 1) * 256] = mm(wha[k], crows[c], TN).astype(BF)
        return carry

    lax.fori_loop(0, 4, dgrad, 0)
    gdin[t] = gds[t]
    g_copies = [
        remote(gds.at[k], gdin.at[t], v_s.at[i], v_r.at[i], (ep, k))
        for i, k in enumerate((right, left, far))
    ]
    begin(g_copies)
    combine(0)
    reduced(2)
    combine(1)
    wgrads(6, 8)
    n_copies = everyone(rnall, n_s, n_r)
    begin(n_copies)
    reduced(3)
    drain(retr.at[most], br_r)
    lane2 = lax.broadcasted_iota(I32, (RELAY, 128), 1)
    rtb[...] = jnp.where(lane2 == 0, mm(c0[...], backr[...]), mm(c1[...], backr[...])).astype(BF)
    home(rtb, srcr, zr_s, zr_r)
    srcr[seat(grp), :] = rtb[0:SEAT, :]
    combine(2)

    landed(n_copies)
    norms = ((rnall[0] + rnall[1]) + rnall[2]) + rnall[3]
    gr_ref[...] = norms[0:16, :]
    ur_ref[...] = norms[16:32, :]
    landed(g_copies)
    total = jnp.zeros((128, 128), F32)
    for k in range(4):
        gdr[:, k * 512 : (k + 1) * 512] = gdin[k]
        sq = jnp.square(gdin[k].astype(F32))
        total += sq[:, 0:128] + sq[:, 128:256] + sq[:, 256:384] + sq[:, 384:512]
    dr_ref[...] = mm(ones16, total, NT, lax.Precision.HIGHEST)[0:1, :]
    combine(3)

    three = pl.ds(0, 3 * SEAT)
    drain(rtb.at[three], zr_r)
    rg_ref[...] = mm(srcr[...], t1[...], TN)[0:2, :].astype(BF)

    drain(sendmeta.at[three], zm_s)
    for i, (q0, n) in enumerate(CHUNKS):
        drain(sendbuf.at[pl.ds(q0, n), three], z_s.at[i])
        drain(pairbuf.at[pl.ds(q0, n), most], y_s.at[i])
    for i in range(4):
        left_here(x_copies(i))
        left_here(f_copies(i))
    drain(scbuf.at[most], ys_s)
    for group in (exch, h_near, h_far, r_copies, n_copies, g_copies):
        left_here(group)
    for p in range(5):
        left_here(s1_copies(p))
        left_here(d_copies(p))
        left_here(s2_copies(p))
    for p in range(4):
        drain(ret.at[p, most], b_s.at[p])
        drain(tokbuf.at[p, three], zb_s.at[p])
    drain(retr.at[most], br_s)
    drain(rtb.at[three], zr_s)
    for p in range(4):
        drain(tokbuf.at[p, three], zb_r.at[p])
        tg_ref[:, p * 128 : (p + 1) * 128] = mm(t1[...], srcv[p], TN).astype(BF)


def store(*refs):
    sems = refs[16]
    copies = [pltpu.make_async_copy(refs[i], refs[8 + i], sems.at[i]) for i in range(8)]
    for c in copies:
        c.start()
    for c in copies:
        c.wait()


def on_device(tokens, expert_ids, route_weights, cotangent, w_gate, w_up, w_down):
    vmem = pl.BlockSpec(memory_space=pltpu.VMEM)
    hbm = pl.BlockSpec(memory_space=pl.ANY)
    dma = pltpu.SemaphoreType.DMA
    v = pltpu.VMEM
    scratch = [
        v((TOK, 1024), BF),
        v((RELAY, TOK), BF),
        v((8, RELAY, 128), BF),
        v((RELAY, 128), BF),
        v((8, RELAY, 128), BF),
        v((RELAY, 128), BF),
        v((SLOTS, RELAY), BF),
        v((8, SLOTS, 128), BF),
        v((SLOTS, 128), BF),
        v((4, 4, SLOTS, 128), BF),
        v((4, SLOTS, 128), BF),
        v((SLOTS, 128), BF),
        v((2048, 256), BF),
        v((4, 128, 512), BF),
        v((SLOTS, 256), F32),
        v((4, SLOTS, 128), F32),
        v((SLOTS, 256), BF),
        v((4, SLOTS, 128), BF),
        v((SLOTS, 128), F32),
        v((4, 8, SLOTS), F32),
        v((4, 5, SLOTS, 128), BF),
        *[v((5, 256, 128), BF) for _ in range(8)],
        v((4, SLOTS, 128), BF),
        v((SLOTS, 128), BF),
        v((4, SLOTS, 128), BF),
        v((SLOTS, 128), BF),
        v((RELAY, SLOTS), BF),
        v((RELAY, SLOTS), BF),
        v((RELAY, SLOTS), BF),
        v((4, RELAY, 128), BF),
        v((RELAY, 128), BF),
        v((4, RELAY, 128), BF),
        v((RELAY, 128), BF),
        v((4, 128, 512), BF),
        v((4, 128, 512), BF),
        v((4, 32, 128), F32),
        v((2, TOK), I32),
        v((2, TOK), BF),
        dma((4,)), dma((3,)),
        dma((6,)), dma((6,)), dma(()), dma(()),
        dma((6,)), dma((6,)), dma(()), dma(()),
        dma((4, 4)), dma((4, 4)),
        dma((4,)), dma((4,)),
        dma((3,)), dma((3,)),
        dma((3,)), dma((3,)),
        dma((3,)), dma((3,)),
        dma((5, 6)), dma((5, 6)),
        dma((4,)), dma((4,)), dma(()), dma(()),
        dma((4,)), dma((4,)), dma(()), dma(()),
        dma((3,)), dma((3,)),
    ]
    outs = (
        v((TOK, 512), BF), v((2, TOK), BF), v((2048, 128), BF), v((2048, 128), BF),
        v((128, 2048), BF), v((16, 128), F32), v((16, 128), F32), v((1, 128), F32),
    )
    held = pl.pallas_call(
        kernel,
        out_shape=outs,
        in_specs=[hbm] * 7,
        out_specs=(vmem,) * 8,
        scratch_shapes=scratch,
        compiler_params=pltpu.CompilerParams(collective_id=0, has_side_effects=True),
    )(expert_ids.T, route_weights.T, tokens, cotangent, w_gate[0], w_up[0], w_down[0])
    tg, rg, gg, gu, gd, gr, ur, dr = pl.pallas_call(
        store,
        out_shape=tuple(jax.ShapeDtypeStruct(o.shape, o.dtype) for o in outs),
        in_specs=[vmem] * 8,
        out_specs=(hbm,) * 8,
        scratch_shapes=[dma((8,))],
    )(*[pltpu.with_memory_space_constraint(h, pltpu.VMEM) for h in held])
    return (
        tg, rg.T, gg[None], gu[None], gd[None],
        gr.reshape(1, 2048), ur.reshape(1, 2048), dr,
    )


def solution(mesh):
    return jax.shard_map(
        on_device,
        mesh=mesh,
        in_specs=(
            P("ep", None), P("ep", None), P("ep", None), P("ep", None),
            P("ep", None, "tp"), P("ep", None, "tp"), P("ep", "tp", None),
        ),
        out_specs=(
            P("ep", "tp"), P("ep", None), P("ep", None, "tp"), P("ep", None, "tp"),
            P("ep", "tp", None), P("ep", None), P("ep", None), P("ep", "tp"),
        ),
        check_vma=False,
    )
```

```python
import functools

import jax
import jax.numpy as jnp
from jax import lax
from jax.experimental import pallas as pl
from jax.experimental.pallas import tpu as pltpu
from jax.sharding import PartitionSpec as P

MESH = pl.DeviceIdType.MESH
BF = jnp.bfloat16
F32 = jnp.float32
I32 = jnp.int32

PLANES = 8
ROW = 16
GROUP = 32
TOK = 128
SEAT = 64
RELAY = 4 * SEAT
SLOTS = 512
BLK = 16
CHUNKS = ((0, 1), (1, 1), (2, 1), (3, 1), (4, 2), (6, 2))
NN = (((1,), (0,)), ((), ()))
NT = (((1,), (1,)), ((), ()))
TN = (((0,), (0,)), ((), ()))


def mm(a, b, dims=NN, precision=None):
    return lax.dot_general(a, b, dims, precision=precision, preferred_element_type=F32)


def kernel(
    ids_hbm, rw_hbm, tok_hbm, cot_hbm, wg_hbm, wu_hbm, wd_hbm,
    tg_ref, rg_ref, ggb, gub, gdr, gr_ref, ur_ref, dr_ref,
    xc, t1, sendbuf, sendmeta, relay, zmeta, p2, pairbuf, scbuf, scin, xs, cs, scr,
    wgu, wdd, wp, wq, acc_gu, acc_hb, hbp, hbr, cot, cotp, cotq, wha, rp, rall, ts, rsv, own, ret, retr, back, backr, c01, c0, c1,
    tokbuf, rtb, srcv, srcr, gds, gdin, rnall, ids_v, rw_v,
    ld_s, w_s, z_s, z_r, zm_s, zm_r, y_s, y_r, ys_s, ys_r, x_s, x_r, h_s, h_r, v_s, v_r, e_s, e_r, u_s, u_r, k_s, k_r, c_s, c_r,
    r_s, r_r, s_s, s_r, b_s, b_r, br_s, br_r, zb_s, zb_r, zr_s, zr_r, n_s, n_r,
):
    ep = lax.axis_index("ep")
    t = lax.axis_index("tp")
    z = ep // ROW
    yc = ep % ROW
    sg = 1 - 2 * (z % 2)
    grp = z // 2
    base = grp * GROUP
    loc = ep % GROUP
    right = (t + 1) % 4
    left = (t + 3) % 4
    far = (t + 2) % 4
    one = t + 1 - 2 * (t % 2)
    two = 3 - t

    def plane(off):
        return ((z + off + PLANES) % PLANES) * ROW + yc

    out_z = [plane(-sg), plane(2 * sg), plane(-3 * sg)]
    in_z = [plane(-sg), plane(-2 * sg), plane(-3 * sg)]

    def remote(src, dst, ssem, rsem, dev):
        return pltpu.make_async_remote_copy(
            src_ref=src, dst_ref=dst, send_sem=ssem, recv_sem=rsem,
            device_id=dev, device_id_type=MESH,
        )

    def drain(ref, sem):
        pltpu.make_async_copy(ref, ref, sem).wait()

    def begin(copies):
        for c in copies:
            c.start()

    def landed(copies):
        for c in copies:
            c.wait_recv()

    def left_here(copies):
        for c in copies:
            c.wait_send()

    def peer(o):
        return (loc + o) % GROUP

    def rows16(i):
        return pl.ds(pl.multiple_of(i * BLK, BLK), BLK)

    def seat(i):
        return pl.ds(pl.multiple_of(i * SEAT, SEAT), SEAT)

    def block(k):
        return pl.ds(pl.multiple_of(k * 512, 512), 512)

    barrier = pltpu.get_barrier_semaphore()

    def hello(e, k):
        pl.semaphore_signal(barrier, inc=1, device_id=(e, k), device_id_type=MESH)

    for e in (plane(-3 * sg), plane(2), plane(-2), plane(-sg)):
        hello(e, t)

    route_in = [
        pltpu.make_async_copy(ids_hbm, ids_v, ld_s.at[2]),
        pltpu.make_async_copy(rw_hbm, rw_v, ld_s.at[3]),
    ]
    begin(route_in)
    ld = [
        pltpu.make_async_copy(tok_hbm.at[:, block(t)], xc.at[:, pl.ds(0, 512)], ld_s.at[0]),
        pltpu.make_async_copy(cot_hbm.at[:, block(t)], xc.at[:, pl.ds(512, 512)], ld_s.at[1]),
    ]
    wl = [
        pltpu.make_async_copy(wg_hbm, wgu.at[:, pl.ds(0, 128)], w_s.at[0]),
        pltpu.make_async_copy(wu_hbm, wgu.at[:, pl.ds(128, 128)], w_s.at[1]),
        pltpu.make_async_copy(wd_hbm.at[:, block(t)], wdd.at[t], w_s.at[2]),
    ]
    begin(ld)

    for k in (far, right, left):
        hello(ep, k)

    def hello_group(o, carry):
        hello(base + peer(o), t)
        return carry

    lax.fori_loop(1, GROUP, hello_group, 0)

    for c in route_in:
        c.wait()
    ids = ids_v[...]
    id0, id1 = ids[0:1, :], ids[1:2, :]
    sub = lax.broadcasted_iota(I32, (TOK, TOK), 0)
    lane = lax.broadcasted_iota(I32, (TOK, TOK), 1)
    oh0 = jnp.where(sub == id0, 1.0, 0.0)
    oh1 = jnp.where(sub == id1, 1.0, 0.0)
    upper = jnp.where(sub < lane, 1.0, 0.0).astype(BF)
    before = mm((oh0 + oh1).astype(BF), upper)
    k0 = jnp.sum(before * oh0, axis=0, keepdims=True)
    k1 = jnp.sum(before * oh1, axis=0, keepdims=True)
    g = id0 // GROUP
    ohg = jnp.where(lax.broadcasted_iota(I32, (16, TOK), 0) == g, 1.0, 0.0)
    q = jnp.sum(mm(ohg.astype(BF), upper) * ohg, axis=0, keepdims=True)
    slot = g * SEAT + q.astype(I32)
    code0 = ((id0 - g * GROUP) * 4).astype(F32) + k0
    code1 = ((id1 - g * GROUP) * 4).astype(F32) + k1
    rw = rw_v[...].astype(F32)
    mrow = jnp.where(
        sub == 0, code0,
        jnp.where(sub == 1, code1, jnp.where(sub == 2, rw[0:1, :], jnp.where(sub == 3, rw[1:2, :], 0.0))),
    ).astype(BF)
    t1[...] = jnp.where(lax.broadcasted_iota(I32, (RELAY, TOK), 0) == slot, 1.0, 0.0).astype(BF)
    sendmeta[...] = mm(t1[...], mrow, NT).astype(BF)
    for c in ld:
        c.wait()
    for h in range(4):
        part = mm(t1[...], xc[:, h * 256 : (h + 1) * 256]).astype(BF)
        sendbuf[2 * h] = part[:, 0:128]
        sendbuf[2 * h + 1] = part[:, 128:256]

    pl.semaphore_wait(barrier, 3 + 4 + GROUP - 1)

    def send_meta():
        for d in (1, 2, 3):
            dst = out_z[d - 1]
            here = pl.ds(d * SEAT, SEAT)
            remote(sendmeta.at[seat(dst // GROUP)], zmeta.at[here], zm_s, zm_r, (dst, t)).start()

    def send_z(i):
        qs = pl.ds(*CHUNKS[i])
        for d in (1, 2, 3):
            dst = out_z[d - 1]
            here = pl.ds(d * SEAT, SEAT)
            remote(
                sendbuf.at[qs, seat(dst // GROUP)], relay.at[qs, here], z_s.at[i], z_r.at[i], (dst, t)
            ).start()

    exch = [
        remote(wd_hbm.at[:, block(k)], wdd.at[t], e_s.at[i], e_r.at[i], (ep, k))
        for i, k in enumerate((right, left, far))
    ]
    send_meta()
    send_z(0)
    send_z(1)
    begin(wl)
    begin(exch)
    zmeta[0:SEAT, :] = sendmeta[seat(grp), :]
    for h in range(8):
        relay[h, 0:SEAT, :] = sendbuf[h, seat(grp), :]
    for c in wl:
        c.wait()
    swap = [
        remote(wgu.at[block(two)], wq.at[0], u_s.at[0], u_r.at[0], (ep, two)),
        remote(wgu.at[block(one)], wp.at[0], u_s.at[1], u_r.at[1], (ep, one)),
        remote(wgu.at[block(far)], wq.at[1], u_s.at[2], u_r.at[2], (ep, two)),
        remote(wgu.at[block(far)], wp.at[1], u_s.at[3], u_r.at[3], (ep, one)),
    ]
    begin(swap)

    drain(zmeta.at[pl.ds(SEAT, 3 * SEAT)], zm_r)
    send_z(2)
    pick = jnp.where(
        lax.broadcasted_iota(I32, (16, 128), 0) == lax.broadcasted_iota(I32, (16, 128), 1), 1.0, 0.0
    ).astype(BF)
    flat = mm(pick, zmeta[...], NT)
    seatrow = lax.broadcasted_iota(I32, (1, RELAY), 1) // SEAT

    def place(code, where_seat):
        code = code.astype(I32)
        return (code // 4) * BLK + where_seat * 4 + code % 4

    pos0 = place(flat[0:1, :], seatrow)
    pos1 = place(flat[1:2, :], seatrow)

    def spread(i, carry):
        at = pl.ds(pl.multiple_of(i * 128, 128), 128)
        p = lax.broadcasted_iota(I32, (128, RELAY), 0) + i * 128
        e0, e1 = p == pos0, p == pos1
        p2[at, :] = jnp.where(e0, 1.0, jnp.where(e1, 1.0, 0.0)).astype(BF)
        return carry

    lax.fori_loop(0, 4, spread, 0)

    def send_group(src, dst, ssem, rsem):
        def body(o, carry):
            e = peer(o)
            remote(src(rows16(e)), dst(rows16(loc)), ssem, rsem, (base + e, t)).start()
            return carry

        lax.fori_loop(1, GROUP, body, 0)

    mine = rows16(loc)
    most = pl.ds(0, (GROUP - 1) * BLK)

    def relay_step(i):
        q0, n = CHUNKS[i]
        drain(relay.at[pl.ds(q0, n), pl.ds(SEAT, 3 * SEAT)], z_r.at[i])
        rows = relay[q0] if n == 1 else jnp.concatenate([relay[q0], relay[q0 + 1]], axis=1)
        out = mm(p2[...], rows).astype(BF)
        for k in range(n):
            pairbuf[q0 + k] = out[:, k * 128 : (k + 1) * 128]
        qs = pl.ds(q0, n)
        if q0 < 4:
            send_group(
                lambda r: pairbuf.at[qs, r], lambda r: xs.at[t, qs, r], y_s.at[i], y_r.at[i]
            )
            for k in range(n):
                xs[t, q0 + k, mine, :] = pairbuf[q0 + k, mine, :]
        else:
            qc = pl.ds(q0 - 4, n)
            send_group(
                lambda r: pairbuf.at[qs, r], lambda r: cs.at[qc, r], y_s.at[i], y_r.at[i]
            )
            for k in range(n):
                cs[q0 - 4 + k, mine, :] = pairbuf[q0 + k, mine, :]

    def routed(i):
        drain(pairbuf.at[pl.ds(*CHUNKS[i]), most], y_r.at[i])

    half0, half1 = pl.ds(0, 256), pl.ds(256, 256)

    def x_copies(i):
        qs = pl.ds(*CHUNKS[i])
        return (
            remote(xs.at[t, qs], xs.at[t, qs], x_s.at[i, 0], x_r.at[i, 0], (ep, right)),
            remote(xs.at[t, qs], xs.at[t, qs], x_s.at[i, 1], x_r.at[i, 1], (ep, left)),
        )

    def f_copies(i):
        qs = pl.ds(*CHUNKS[i])
        return (
            remote(xs.at[left, qs, half0], xs.at[left, qs, half0], x_s.at[i, 2], x_r.at[i, 2], (ep, right)),
            remote(xs.at[right, qs, half1], xs.at[right, qs, half1], x_s.at[i, 3], x_r.at[i, 3], (ep, left)),
        )

    def forward_step(i):
        landed(x_copies(i))
        begin(f_copies(i))

    def product(k, i, first=False):
        q0, n = CHUNKS[i]
        at = pl.ds(pl.multiple_of(k * 512 + q0 * 128, 128), n * 128)
        rows = xs[k, q0] if n == 1 else jnp.concatenate([xs[k, q0], xs[k, q0 + 1]], axis=1)
        part = mm(rows, wgu[at, :])
        if first:
            acc_gu[...] = part
        else:
            acc_gu[...] += part

    def near_products(i):
        def body(j, carry):
            product((t + 1 + 2 * j) % 4, i)
            return carry

        lax.fori_loop(0, 2, body, 0)

    def hb_part(c, first):
        rows = jnp.concatenate([cs[2 * c], cs[2 * c + 1]], axis=1)

        def body(k, carry):
            part = mm(rows, wdd[k, :, c * 256 : (c + 1) * 256], NT)
            if first:
                acc_hb[k] = part
            else:
                whole = acc_hb[k] + part
                acc_hb[k] = whole
                hbp[k] = whole.astype(BF)
            return carry

        lax.fori_loop(0, 4, body, 0)

    relay_step(0)
    relay_step(1)
    send_z(3)
    send_z(4)
    routed(0)
    begin(x_copies(0))
    product(t, 0, first=True)
    relay_step(2)
    send_z(5)

    seatcol = lax.broadcasted_iota(I32, (RELAY, 1), 0) // SEAT
    codes = zmeta[...].astype(F32)
    lanes = lax.broadcasted_iota(I32, (RELAY, 128), 1)

    def weight_rows(k):
        code = codes[:, k : k + 1].astype(I32)
        to = jnp.where(lanes == code // 4, 1.0, 0.0).astype(BF)
        at = jnp.where(lanes == seatcol * 4 + code % 4, codes[:, k + 2 : k + 3], 0.0).astype(BF)
        return mm(to, at, TN)

    table = weight_rows(0) + weight_rows(1)
    for e in range(GROUP):
        scbuf[e] = table[e : e + 1, :]

    def send_weights(o, carry):
        e = peer(o)
        remote(scbuf.at[e], scin.at[loc], ys_s, ys_r, (base + e, t)).start()
        return carry

    lax.fori_loop(1, GROUP, send_weights, 0)
    scin[loc] = scbuf[loc]
    routed(1)
    begin(x_copies(1))
    product(t, 1)
    relay_step(3)
    relay_step(4)
    routed(2)
    begin(x_copies(2))
    product(t, 2)
    forward_step(0)
    near_products(0)
    routed(3)
    begin(x_copies(3))
    product(t, 3)
    relay_step(5)

    back0 = place(codes[:, 0:1], seatcol)
    back1 = place(codes[:, 1:2], seatcol)
    wide = lax.broadcasted_iota(I32, (RELAY, SLOTS), 1)
    m0 = jnp.where(wide == back0, 1.0, 0.0)
    m1 = jnp.where(wide == back1, 1.0, 0.0)
    c0[...] = m0.astype(BF)
    c1[...] = m1.astype(BF)
    c01[...] = (m0 + m1).astype(BF)

    forward_step(1)
    near_products(1)
    landed(exch)
    forward_step(2)
    near_products(2)
    routed(4)
    hb_part(0, True)
    landed(f_copies(0))
    product(far, 0)
    forward_step(3)
    routed(5)
    hb_part(1, False)
    k_copies = [
        remote(hbp.at[k], hbr.at[i], k_s.at[i], k_r.at[i], (ep, k))
        for i, k in enumerate((far, right, left))
    ]
    begin(k_copies)
    near_products(3)
    for i in (1, 2, 3):
        landed(f_copies(i))
        product(far, i)

    drain(scbuf.at[pl.ds(0, GROUP - 1)], ys_r)
    prow = lax.broadcasted_iota(I32, (SLOTS, GROUP), 0)
    from_relay = jnp.where(prow // BLK == lax.broadcasted_iota(I32, (SLOTS, GROUP), 1), 1.0, 0.0)
    listed = mm(from_relay.astype(BF), scin[:, 0, :].astype(BF))
    inside = lax.broadcasted_iota(I32, (SLOTS, 128), 0) % BLK == lax.broadcasted_iota(I32, (SLOTS, 128), 1)
    scr[...] = mm(jnp.where(inside, listed, 0.0).astype(BF), jnp.ones((128, 128), BF))

    def hiddens(i, carry):
        at = pl.ds(pl.multiple_of(i * 64, 64), 64)
        gate, up = acc_gu[at, 0:128], acc_gu[at, 128:256]
        hid = gate * jax.nn.sigmoid(gate) * up
        wha[t, at, :] = (scr[at, :] * hid).astype(BF)
        return carry

    lax.fori_loop(0, 8, hiddens, 0)
    landed(k_copies)

    def activate(i, carry):
        at = pl.ds(pl.multiple_of(i * 64, 64), 64)
        gate, up = acc_gu[at, 0:128], acc_gu[at, 128:256]
        hb = acc_hb[t, at, :] + hbr[0, at, :].astype(F32)
        hb = hb + hbr[1, at, :].astype(F32) + hbr[2, at, :].astype(F32)
        sc = scr[at, :]
        sig = jax.nn.sigmoid(gate)
        act = gate * sig
        hc = sc * hb
        cot[at, 0:128] = (hc * up * sig * (1.0 + gate * (1.0 - sig))).astype(BF)
        cot[at, 128:256] = (hc * act).astype(BF)
        rp[at, :] = act * up * hb
        return carry

    lax.fori_loop(0, 8, activate, 0)

    def everyone(buf, ssem, rsem):
        return [
            remote(buf.at[t], buf.at[t], ssem.at[i], rsem.at[i], (ep, k))
            for i, k in enumerate((right, left, far))
        ]

    c_copies = [
        remote(cot.at[half0], cotp, c_s.at[0], c_r.at[0], (ep, one)),
        remote(cot.at[half1], cotq, c_s.at[1], c_r.at[1], (ep, two)),
    ]
    begin(c_copies)
    ones16 = jnp.ones((16, 128), F32)
    rsum = mm(ones16, rp[...], NT, lax.Precision.HIGHEST)
    rall[t] = rsum[0:8, :]

    def partial(rows, mine_at, near, near_w, p):
        at = pl.ds(pl.multiple_of(mine_at * 512 + p * 256, 256), 256)
        part = mm(cot[rows], wgu[at, :], NT)
        return part + mm(near[...], near_w[p * 256 : (p + 1) * 256, :], NT)

    def away(p):
        top = partial(slice(0, 256), two, cotp, wp[1], p).astype(BF)
        low = partial(slice(256, 512), one, cotq, wq[1], p).astype(BF)
        for k in range(2):
            ts[0, 2 * p + k] = top[:, k * 128 : (k + 1) * 128]
            ts[1, 2 * p + k] = low[:, k * 128 : (k + 1) * 128]

    def kept(p):
        top = partial(slice(0, 256), t, cotp, wp[0], p)
        low = partial(slice(256, 512), t, cotq, wq[0], p)
        for k in range(2):
            own[2 * p + k, 0:256, :] = top[:, k * 128 : (k + 1) * 128]
            own[2 * p + k, 256:512, :] = low[:, k * 128 : (k + 1) * 128]

    def t_copies(p):
        return (
            remote(ts.at[0, p], rsv.at[0, p], s_s.at[p, 0], s_r.at[p, 0], (ep, two)),
            remote(ts.at[1, p], rsv.at[1, p], s_s.at[p, 1], s_r.at[p, 1], (ep, one)),
        )

    def wgrad(j):
        k, h = j // 2, j % 2
        at = pl.ds(pl.multiple_of(j * 256, 256), 256)
        rows = jnp.concatenate([xs[k, 2 * h], xs[k, 2 * h + 1]], axis=1)
        both = mm(rows, cot[...], TN).astype(BF)
        ggb[at, :] = both[:, 0:128]
        gub[at, :] = both[:, 128:256]
        sq = jnp.square(both.astype(F32))
        ng = mm(ones16, sq[:, 0:128], NT, lax.Precision.HIGHEST)
        nu = mm(ones16, sq[:, 128:256], NT, lax.Precision.HIGHEST)
        rnall[t, pl.ds(2 * j, 1), :] = ng[0:1, 0:128]
        rnall[t, pl.ds(2 * j + 1, 1), :] = ng[0:1, 128:256]
        rnall[t, pl.ds(16 + 2 * j, 1), :] = nu[0:1, 0:128]
        rnall[t, pl.ds(17 + 2 * j, 1), :] = nu[0:1, 128:256]

    def wgrads(lo, hi):
        def body(j, carry):
            wgrad(j)
            return carry

        lax.fori_loop(lo, hi, body, 0)

    def reduced(p):
        landed(t_copies(p))
        ret[p, 0:256, :] = (own[p, 0:256, :] + rsv[0, p].astype(F32)).astype(BF)
        ret[p, 256:512, :] = (own[p, 256:512, :] + rsv[1, p].astype(F32)).astype(BF)
        send_group(lambda r: ret.at[p, r], lambda r: back.at[p, r], b_s.at[p], b_r.at[p])
        back[p, mine, :] = ret[p, mine, :]

    def home(src, dst, ssem, rsem):
        for d in (1, 2, 3):
            remote(src.at[pl.ds(d * SEAT, SEAT)], dst.at[seat(grp)], ssem, rsem, (in_z[d - 1], t)).start()

    def combine(p):
        drain(ret.at[p, most], b_r.at[p])
        tokbuf[p] = mm(c01[...], back[p]).astype(BF)
        home(tokbuf.at[p], srcv.at[p], zb_s.at[p], zb_r.at[p])
        srcv[p, seat(grp), :] = tokbuf[p, 0:SEAT, :]

    r_copies = everyone(rall, r_s, r_r)
    begin(r_copies)
    wgrads(0, 2)
    h_near = (
        remote(wha.at[t], wha.at[t], h_s.at[0], h_r.at[0], (ep, right)),
        remote(wha.at[t], wha.at[t], h_s.at[1], h_r.at[1], (ep, left)),
    )
    h_far = (
        remote(wha.at[left, half0], wha.at[left, half0], h_s.at[2], h_r.at[2], (ep, right)),
        remote(wha.at[right, half1], wha.at[right, half1], h_s.at[3], h_r.at[3], (ep, left)),
    )
    begin(h_near)
    landed(swap)
    landed(c_copies)
    away(0)
    begin(t_copies(0))
    away(1)

    landed(r_copies)
    rtot = ((rall[0] + rall[1]) + rall[2]) + rall[3]
    rtot = jnp.where(lax.broadcasted_iota(I32, (8, SLOTS), 0) == 0, rtot, 0.0)
    retr[...] = mm(rtot.astype(BF), jnp.ones((8, 128), BF), TN).astype(BF)
    begin(t_copies(1))
    send_group(lambda r: retr.at[r], lambda r: backr.at[r], br_s, br_r)
    backr[mine, :] = retr[mine, :]
    kept(0)
    begin(t_copies(2))
    landed(h_near)
    begin(h_far)
    reduced(0)
    begin(t_copies(3))
    kept(1)
    wgrads(2, 3)
    reduced(1)

    landed(h_far)
    crows = [jnp.concatenate([cs[0], cs[1]], axis=1), jnp.concatenate([cs[2], cs[3]], axis=1)]

    def dgrad(k, carry):
        for c in range(2):
            gds[k, :, c * 256 : (c + 1) * 256] = mm(wha[k], crows[c], TN).astype(BF)
        return carry

    lax.fori_loop(0, 4, dgrad, 0)
    gdin[t] = gds[t]
    g_copies = [
        remote(gds.at[k], gdin.at[t], v_s.at[i], v_r.at[i], (ep, k))
        for i, k in enumerate((far, right, left))
    ]
    begin(g_copies)
    reduced(2)
    wgrads(3, 5)
    reduced(3)
    combine(0)
    wgrads(5, 8)
    n_copies = everyone(rnall, n_s, n_r)
    begin(n_copies)
    combine(1)
    drain(retr.at[most], br_r)
    lane2 = lax.broadcasted_iota(I32, (RELAY, 128), 1)
    rtb[...] = jnp.where(lane2 == 0, mm(c0[...], backr[...]), mm(c1[...], backr[...])).astype(BF)
    home(rtb, srcr, zr_s, zr_r)
    srcr[seat(grp), :] = rtb[0:SEAT, :]
    landed(n_copies)
    norms = ((rnall[0] + rnall[1]) + rnall[2]) + rnall[3]
    gr_ref[...] = norms[0:16, :]
    ur_ref[...] = norms[16:32, :]
    combine(2)
    combine(3)
    landed(g_copies)
    total = jnp.zeros((128, 128), F32)
    for k in range(4):
        gdr[:, k * 512 : (k + 1) * 512] = gdin[k]
        sq = jnp.square(gdin[k].astype(F32))
        total += sq[:, 0:128] + sq[:, 128:256] + sq[:, 256:384] + sq[:, 384:512]
    dr_ref[...] = mm(ones16, total, NT, lax.Precision.HIGHEST)[0:1, :]

    three = pl.ds(0, 3 * SEAT)
    drain(rtb.at[three], zr_r)
    rg_ref[...] = mm(srcr[...], t1[...], TN)[0:2, :].astype(BF)

    drain(sendmeta.at[three], zm_s)
    for i, (q0, n) in enumerate(CHUNKS):
        drain(sendbuf.at[pl.ds(q0, n), three], z_s.at[i])
        drain(pairbuf.at[pl.ds(q0, n), most], y_s.at[i])
    for i in range(4):
        left_here(x_copies(i))
        left_here(f_copies(i))
    drain(scbuf.at[pl.ds(0, GROUP - 1)], ys_s)
    for group in (exch, swap, k_copies, c_copies, h_near, h_far, r_copies, n_copies, g_copies):
        left_here(group)
    for p in range(4):
        left_here(t_copies(p))
        drain(ret.at[p, most], b_s.at[p])
        drain(tokbuf.at[p, three], zb_s.at[p])
    drain(retr.at[most], br_s)
    drain(rtb.at[three], zr_s)
    for p in range(4):
        drain(tokbuf.at[p, three], zb_r.at[p])
        tg_ref[:, p * 128 : (p + 1) * 128] = mm(t1[...], srcv[p], TN).astype(BF)


def store(*refs):
    sems = refs[16]
    copies = [pltpu.make_async_copy(refs[i], refs[8 + i], sems.at[i]) for i in range(8)]
    for c in copies:
        c.start()
    for c in copies:
        c.wait()


def on_device(tokens, expert_ids, route_weights, cotangent, w_gate, w_up, w_down):
    vmem = pl.BlockSpec(memory_space=pltpu.VMEM)
    hbm = pl.BlockSpec(memory_space=pl.ANY)
    dma = pltpu.SemaphoreType.DMA
    v = pltpu.VMEM
    scratch = [
        v((TOK, 1024), BF),
        v((RELAY, TOK), BF),
        v((8, RELAY, 128), BF),
        v((RELAY, 128), BF),
        v((8, RELAY, 128), BF),
        v((RELAY, 128), BF),
        v((SLOTS, RELAY), BF),
        v((8, SLOTS, 128), BF),
        v((GROUP, 1, 128), F32),
        v((GROUP, 1, 128), F32),
        v((4, 4, SLOTS, 128), BF),
        v((4, SLOTS, 128), BF),
        v((SLOTS, 128), F32),
        v((2048, 256), BF),
        v((4, 128, 512), BF),
        v((2, 512, 256), BF),
        v((2, 512, 256), BF),
        v((SLOTS, 256), F32),
        v((4, SLOTS, 128), F32),
        v((4, SLOTS, 128), BF),
        v((3, SLOTS, 128), BF),
        v((SLOTS, 256), BF),
        v((256, 256), BF),
        v((256, 256), BF),
        v((4, SLOTS, 128), BF),
        v((SLOTS, 128), F32),
        v((4, 8, SLOTS), F32),
        v((2, 4, 256, 128), BF),
        v((2, 4, 256, 128), BF),
        v((4, SLOTS, 128), F32),
        v((4, SLOTS, 128), BF),
        v((SLOTS, 128), BF),
        v((4, SLOTS, 128), BF),
        v((SLOTS, 128), BF),
        v((RELAY, SLOTS), BF),
        v((RELAY, SLOTS), BF),
        v((RELAY, SLOTS), BF),
        v((4, RELAY, 128), BF),
        v((RELAY, 128), BF),
        v((4, RELAY, 128), BF),
        v((RELAY, 128), BF),
        v((4, 128, 512), BF),
        v((4, 128, 512), BF),
        v((4, 32, 128), F32),
        v((2, TOK), I32),
        v((2, TOK), BF),
        dma((4,)), dma((3,)),
        dma((6,)), dma((6,)), dma(()), dma(()),
        dma((6,)), dma((6,)), dma(()), dma(()),
        dma((4, 4)), dma((4, 4)),
        dma((4,)), dma((4,)),
        dma((3,)), dma((3,)),
        dma((3,)), dma((3,)),
        dma((4,)), dma((4,)),
        dma((3,)), dma((3,)),
        dma((2,)), dma((2,)),
        dma((3,)), dma((3,)),
        dma((4, 2)), dma((4, 2)),
        dma((4,)), dma((4,)), dma(()), dma(()),
        dma((4,)), dma((4,)), dma(()), dma(()),
        dma((3,)), dma((3,)),
    ]
    outs = (
        v((TOK, 512), BF), v((2, TOK), BF), v((2048, 128), BF), v((2048, 128), BF),
        v((128, 2048), BF), v((16, 128), F32), v((16, 128), F32), v((1, 128), F32),
    )
    held = pl.pallas_call(
        kernel,
        out_shape=outs,
        in_specs=[hbm] * 7,
        out_specs=(vmem,) * 8,
        scratch_shapes=scratch,
        compiler_params=pltpu.CompilerParams(collective_id=0, has_side_effects=True),
    )(expert_ids.T, route_weights.T, tokens, cotangent, w_gate[0], w_up[0], w_down[0])
    tg, rg, gg, gu, gd, gr, ur, dr = pl.pallas_call(
        store,
        out_shape=tuple(jax.ShapeDtypeStruct(o.shape, o.dtype) for o in outs),
        in_specs=[vmem] * 8,
        out_specs=(hbm,) * 8,
        scratch_shapes=[dma((8,))],
    )(*[pltpu.with_memory_space_constraint(h, pltpu.VMEM) for h in held])
    return (
        tg, rg.T, gg[None], gu[None], gd[None],
        gr.reshape(1, 2048), ur.reshape(1, 2048), dr,
    )


def solution(mesh):
    return jax.shard_map(
        on_device,
        mesh=mesh,
        in_specs=(
            P("ep", None), P("ep", None), P("ep", None), P("ep", None),
            P("ep", None, "tp"), P("ep", None, "tp"), P("ep", "tp", None),
        ),
        out_specs=(
            P("ep", "tp"), P("ep", None), P("ep", None, "tp"), P("ep", None, "tp"),
            P("ep", "tp", None), P("ep", None), P("ep", None), P("ep", "tp"),
        ),
        check_vma=False,
    )
```

```python
import functools

import jax
import jax.numpy as jnp
from jax import lax
from jax.experimental import pallas as pl
from jax.experimental.pallas import tpu as pltpu
from jax.sharding import PartitionSpec as P

MESH = pl.DeviceIdType.MESH
BF = jnp.bfloat16
F32 = jnp.float32
I32 = jnp.int32

PLANES = 8
ROW = 16
GROUP = 32
TOK = 128
SEAT = 64
RELAY = 4 * SEAT
SLOTS = 512
BLK = 16
CHUNKS = ((0, 1), (1, 1), (2, 1), (3, 1), (4, 2), (6, 2))
NN = (((1,), (0,)), ((), ()))
NT = (((1,), (1,)), ((), ()))
TN = (((0,), (0,)), ((), ()))


def mm(a, b, dims=NN, precision=None):
    return lax.dot_general(a, b, dims, precision=precision, preferred_element_type=F32)


def kernel(
    ids_hbm, rw_hbm, tok_hbm, cot_hbm, wg_hbm, wu_hbm, wd_hbm,
    tg_ref, rg_ref, ggb, gub, gdr, gr_ref, ur_ref, dr_ref,
    xc, t1, sendbuf, sendmeta, relay, zmeta, p2, pairbuf, scbuf, scin, xs, cs, scr,
    wgu, wdd, wp, wq, acc_gu, acc_hb, hbp, hbr, cot, cotp, cotq, wha, rp, rall, ts, rsv, own, ret, retr, back, backr, c01, c0, c1,
    tokbuf, rtb, srcv, srcr, gds, gdin, rnall, ids_v, rw_v,
    ld_s, w_s, z_s, z_r, zm_s, zm_r, y_s, y_r, ys_s, ys_r, x_s, x_r, h_s, h_r, v_s, v_r, e_s, e_r, u_s, u_r, k_s, k_r, c_s, c_r,
    r_s, r_r, s_s, s_r, b_s, b_r, br_s, br_r, zb_s, zb_r, zr_s, zr_r, n_s, n_r,
):
    ep = lax.axis_index("ep")
    t = lax.axis_index("tp")
    z = ep // ROW
    yc = ep % ROW
    sg = 1 - 2 * (z % 2)
    grp = z // 2
    base = grp * GROUP
    loc = ep % GROUP
    right = (t + 1) % 4
    left = (t + 3) % 4
    far = (t + 2) % 4
    one = t + 1 - 2 * (t % 2)
    two = 3 - t

    def plane(off):
        return ((z + off + PLANES) % PLANES) * ROW + yc

    out_z = [plane(-sg), plane(2 * sg), plane(-3 * sg)]
    in_z = [plane(-sg), plane(-2 * sg), plane(-3 * sg)]

    def remote(src, dst, ssem, rsem, dev):
        return pltpu.make_async_remote_copy(
            src_ref=src, dst_ref=dst, send_sem=ssem, recv_sem=rsem,
            device_id=dev, device_id_type=MESH,
        )

    def drain(ref, sem):
        pltpu.make_async_copy(ref, ref, sem).wait()

    def begin(copies):
        for c in copies:
            c.start()

    def landed(copies):
        for c in copies:
            c.wait_recv()

    def left_here(copies):
        for c in copies:
            c.wait_send()

    def peer(o):
        return (loc + o) % GROUP

    def rows16(i):
        return pl.ds(pl.multiple_of(i * BLK, BLK), BLK)

    def seat(i):
        return pl.ds(pl.multiple_of(i * SEAT, SEAT), SEAT)

    def block(k):
        return pl.ds(pl.multiple_of(k * 512, 512), 512)

    barrier = pltpu.get_barrier_semaphore()

    def hello(e, k):
        pl.semaphore_signal(barrier, inc=1, device_id=(e, k), device_id_type=MESH)

    for e in (plane(-3 * sg), plane(2), plane(-2), plane(-sg)):
        hello(e, t)

    route_in = [
        pltpu.make_async_copy(ids_hbm, ids_v, ld_s.at[2]),
        pltpu.make_async_copy(rw_hbm, rw_v, ld_s.at[3]),
    ]
    begin(route_in)
    ld = [
        pltpu.make_async_copy(tok_hbm.at[:, block(t)], xc.at[:, pl.ds(0, 512)], ld_s.at[0]),
        pltpu.make_async_copy(cot_hbm.at[:, block(t)], xc.at[:, pl.ds(512, 512)], ld_s.at[1]),
    ]
    wl = [
        pltpu.make_async_copy(wg_hbm, wgu.at[:, pl.ds(0, 128)], w_s.at[0]),
        pltpu.make_async_copy(wu_hbm, wgu.at[:, pl.ds(128, 128)], w_s.at[1]),
        pltpu.make_async_copy(wd_hbm.at[:, block(t)], wdd.at[t], w_s.at[2]),
    ]
    begin(ld)

    for k in (far, right, left):
        hello(ep, k)

    def hello_group(o, carry):
        hello(base + peer(o), t)
        return carry

    lax.fori_loop(1, GROUP, hello_group, 0)

    for c in route_in:
        c.wait()
    ids = ids_v[...]
    id0, id1 = ids[0:1, :], ids[1:2, :]
    sub = lax.broadcasted_iota(I32, (TOK, TOK), 0)
    lane = lax.broadcasted_iota(I32, (TOK, TOK), 1)
    oh0 = jnp.where(sub == id0, 1.0, 0.0)
    oh1 = jnp.where(sub == id1, 1.0, 0.0)
    upper = jnp.where(sub < lane, 1.0, 0.0).astype(BF)
    before = mm((oh0 + oh1).astype(BF), upper)
    k0 = jnp.sum(before * oh0, axis=0, keepdims=True)
    k1 = jnp.sum(before * oh1, axis=0, keepdims=True)
    g = id0 // GROUP
    ohg = jnp.where(lax.broadcasted_iota(I32, (16, TOK), 0) == g, 1.0, 0.0)
    q = jnp.sum(mm(ohg.astype(BF), upper) * ohg, axis=0, keepdims=True)
    slot = g * SEAT + q.astype(I32)
    code0 = ((id0 - g * GROUP) * 4).astype(F32) + k0
    code1 = ((id1 - g * GROUP) * 4).astype(F32) + k1
    rw = rw_v[...].astype(F32)
    mrow = jnp.where(
        sub == 0, code0,
        jnp.where(sub == 1, code1, jnp.where(sub == 2, rw[0:1, :], jnp.where(sub == 3, rw[1:2, :], 0.0))),
    ).astype(BF)
    t1[...] = jnp.where(lax.broadcasted_iota(I32, (RELAY, TOK), 0) == slot, 1.0, 0.0).astype(BF)
    sendmeta[...] = mm(t1[...], mrow, NT).astype(BF)
    for c in ld:
        c.wait()
    for h in range(4):
        part = mm(t1[...], xc[:, h * 256 : (h + 1) * 256]).astype(BF)
        sendbuf[2 * h] = part[:, 0:128]
        sendbuf[2 * h + 1] = part[:, 128:256]

    pl.semaphore_wait(barrier, 3 + 4 + GROUP - 1)

    def send_meta():
        for d in (1, 2, 3):
            dst = out_z[d - 1]
            here = pl.ds(d * SEAT, SEAT)
            remote(sendmeta.at[seat(dst // GROUP)], zmeta.at[here], zm_s, zm_r, (dst, t)).start()

    def send_z(i):
        qs = pl.ds(*CHUNKS[i])
        for d in (1, 2, 3):
            dst = out_z[d - 1]
            here = pl.ds(d * SEAT, SEAT)
            remote(
                sendbuf.at[qs, seat(dst // GROUP)], relay.at[qs, here], z_s.at[i], z_r.at[i], (dst, t)
            ).start()

    exch = [
        remote(wd_hbm.at[:, block(k)], wdd.at[t], e_s.at[i], e_r.at[i], (ep, k))
        for i, k in enumerate((right, left, far))
    ]
    send_meta()
    send_z(0)
    send_z(1)
    begin(wl)
    begin(exch)
    zmeta[0:SEAT, :] = sendmeta[seat(grp), :]
    for h in range(8):
        relay[h, 0:SEAT, :] = sendbuf[h, seat(grp), :]
    for c in wl:
        c.wait()
    swap = [
        remote(wgu.at[block(two)], wq.at[0], u_s.at[0], u_r.at[0], (ep, two)),
        remote(wgu.at[block(one)], wp.at[0], u_s.at[1], u_r.at[1], (ep, one)),
        remote(wgu.at[block(far)], wq.at[1], u_s.at[2], u_r.at[2], (ep, two)),
        remote(wgu.at[block(far)], wp.at[1], u_s.at[3], u_r.at[3], (ep, one)),
    ]
    begin(swap)

    drain(zmeta.at[pl.ds(SEAT, 3 * SEAT)], zm_r)
    send_z(2)
    pick = jnp.where(
        lax.broadcasted_iota(I32, (16, 128), 0) == lax.broadcasted_iota(I32, (16, 128), 1), 1.0, 0.0
    ).astype(BF)
    flat = mm(pick, zmeta[...], NT)
    seatrow = lax.broadcasted_iota(I32, (1, RELAY), 1) // SEAT

    def place(code, where_seat):
        code = code.astype(I32)
        return (code // 4) * BLK + where_seat * 4 + code % 4

    pos0 = place(flat[0:1, :], seatrow)
    pos1 = place(flat[1:2, :], seatrow)

    def spread(i, carry):
        at = pl.ds(pl.multiple_of(i * 128, 128), 128)
        p = lax.broadcasted_iota(I32, (128, RELAY), 0) + i * 128
        e0, e1 = p == pos0, p == pos1
        p2[at, :] = jnp.where(e0, 1.0, jnp.where(e1, 1.0, 0.0)).astype(BF)
        return carry

    lax.fori_loop(0, 4, spread, 0)

    def send_group(src, dst, ssem, rsem):
        def body(o, carry):
            e = peer(o)
            remote(src(rows16(e)), dst(rows16(loc)), ssem, rsem, (base + e, t)).start()
            return carry

        lax.fori_loop(1, GROUP, body, 0)

    mine = rows16(loc)
    most = pl.ds(0, (GROUP - 1) * BLK)

    def relay_step(i):
        q0, n = CHUNKS[i]
        drain(relay.at[pl.ds(q0, n), pl.ds(SEAT, 3 * SEAT)], z_r.at[i])
        rows = relay[q0] if n == 1 else jnp.concatenate([relay[q0], relay[q0 + 1]], axis=1)
        out = mm(p2[...], rows).astype(BF)
        for k in range(n):
            pairbuf[q0 + k] = out[:, k * 128 : (k + 1) * 128]
        qs = pl.ds(q0, n)
        if q0 < 4:
            send_group(
                lambda r: pairbuf.at[qs, r], lambda r: xs.at[t, qs, r], y_s.at[i], y_r.at[i]
            )
            for k in range(n):
                xs[t, q0 + k, mine, :] = pairbuf[q0 + k, mine, :]
        else:
            qc = pl.ds(q0 - 4, n)
            send_group(
                lambda r: pairbuf.at[qs, r], lambda r: cs.at[qc, r], y_s.at[i], y_r.at[i]
            )
            for k in range(n):
                cs[q0 - 4 + k, mine, :] = pairbuf[q0 + k, mine, :]

    def routed(i):
        drain(pairbuf.at[pl.ds(*CHUNKS[i]), most], y_r.at[i])

    half0, half1 = pl.ds(0, 256), pl.ds(256, 256)

    def x_copies(i):
        qs = pl.ds(*CHUNKS[i])
        return (
            remote(xs.at[t, qs], xs.at[t, qs], x_s.at[i, 0], x_r.at[i, 0], (ep, right)),
            remote(xs.at[t, qs], xs.at[t, qs], x_s.at[i, 1], x_r.at[i, 1], (ep, left)),
        )

    def f_copies(i):
        qs = pl.ds(*CHUNKS[i])
        return (
            remote(xs.at[left, qs, half0], xs.at[left, qs, half0], x_s.at[i, 2], x_r.at[i, 2], (ep, right)),
            remote(xs.at[right, qs, half1], xs.at[right, qs, half1], x_s.at[i, 3], x_r.at[i, 3], (ep, left)),
        )

    def forward_step(i):
        landed(x_copies(i))
        begin(f_copies(i))

    def product(k, i, first=False):
        q0, n = CHUNKS[i]
        at = pl.ds(pl.multiple_of(k * 512 + q0 * 128, 128), n * 128)
        rows = xs[k, q0] if n == 1 else jnp.concatenate([xs[k, q0], xs[k, q0 + 1]], axis=1)
        part = mm(rows, wgu[at, :])
        if first:
            acc_gu[...] = part
        else:
            acc_gu[...] += part

    def near_products(i):
        def body(j, carry):
            product((t + 1 + 2 * j) % 4, i)
            return carry

        lax.fori_loop(0, 2, body, 0)

    def hb_rows(c):
        return jnp.concatenate([cs[2 * c], cs[2 * c + 1]], axis=1)

    def hb_start():
        rows = hb_rows(0)

        def body(k, carry):
            acc_hb[k] = mm(rows, wdd[k, :, 0:256], NT)
            return carry

        lax.fori_loop(0, 4, body, 0)

    def hb_whole(k):
        return acc_hb[k] + mm(hb_rows(1), wdd[k, :, 256:512], NT)

    relay_step(0)
    relay_step(1)
    send_z(3)
    send_z(4)
    routed(0)
    begin(x_copies(0))
    product(t, 0, first=True)
    relay_step(2)
    send_z(5)

    seatcol = lax.broadcasted_iota(I32, (RELAY, 1), 0) // SEAT
    codes = zmeta[...].astype(F32)
    lanes = lax.broadcasted_iota(I32, (RELAY, 128), 1)

    def weight_rows(k):
        code = codes[:, k : k + 1].astype(I32)
        to = jnp.where(lanes == code // 4, 1.0, 0.0).astype(BF)
        at = jnp.where(lanes == seatcol * 4 + code % 4, codes[:, k + 2 : k + 3], 0.0).astype(BF)
        return mm(to, at, TN)

    table = weight_rows(0) + weight_rows(1)
    for e in range(GROUP):
        scbuf[e] = table[e : e + 1, :]

    def send_weights(o, carry):
        e = peer(o)
        remote(scbuf.at[e], scin.at[loc], ys_s, ys_r, (base + e, t)).start()
        return carry

    lax.fori_loop(1, GROUP, send_weights, 0)
    scin[loc] = scbuf[loc]
    routed(1)
    begin(x_copies(1))
    product(t, 1)
    relay_step(3)
    relay_step(4)
    routed(2)
    begin(x_copies(2))
    product(t, 2)
    forward_step(0)
    relay_step(5)
    near_products(0)
    routed(3)
    begin(x_copies(3))
    product(t, 3)

    back0 = place(codes[:, 0:1], seatcol)
    back1 = place(codes[:, 1:2], seatcol)
    wide = lax.broadcasted_iota(I32, (RELAY, SLOTS), 1)
    m0 = jnp.where(wide == back0, 1.0, 0.0)
    m1 = jnp.where(wide == back1, 1.0, 0.0)
    c0[...] = m0.astype(BF)
    c1[...] = m1.astype(BF)
    c01[...] = (m0 + m1).astype(BF)

    forward_step(1)
    near_products(1)
    landed(exch)
    forward_step(2)
    near_products(2)
    routed(4)
    hb_start()
    landed(f_copies(0))
    product(far, 0)
    forward_step(3)
    routed(5)
    k_copies = [
        remote(hbp.at[k], hbr.at[i], k_s.at[i], k_r.at[i], (ep, k))
        for i, k in enumerate((far, right, left))
    ]
    for i, k in enumerate((far, right, left)):
        hbp[k] = hb_whole(k).astype(BF)
        k_copies[i].start()
    acc_hb[t] = hb_whole(t)
    near_products(3)
    for i in (1, 2, 3):
        landed(f_copies(i))
        product(far, i)

    drain(scbuf.at[pl.ds(0, GROUP - 1)], ys_r)
    prow = lax.broadcasted_iota(I32, (SLOTS, GROUP), 0)
    from_relay = jnp.where(prow // BLK == lax.broadcasted_iota(I32, (SLOTS, GROUP), 1), 1.0, 0.0)
    listed = mm(from_relay.astype(BF), scin[:, 0, :].astype(BF))
    inside = lax.broadcasted_iota(I32, (SLOTS, 128), 0) % BLK == lax.broadcasted_iota(I32, (SLOTS, 128), 1)
    scr[...] = mm(jnp.where(inside, listed, 0.0).astype(BF), jnp.ones((128, 128), BF))

    def hiddens(i, carry):
        at = pl.ds(pl.multiple_of(i * 64, 64), 64)
        gate, up = acc_gu[at, 0:128], acc_gu[at, 128:256]
        hid = gate * jax.nn.sigmoid(gate) * up
        wha[t, at, :] = (scr[at, :] * hid).astype(BF)
        return carry

    lax.fori_loop(0, 8, hiddens, 0)
    landed(k_copies)

    def activate(i, carry):
        at = pl.ds(pl.multiple_of(i * 64, 64), 64)
        gate, up = acc_gu[at, 0:128], acc_gu[at, 128:256]
        hb = acc_hb[t, at, :] + hbr[0, at, :].astype(F32)
        hb = hb + hbr[1, at, :].astype(F32) + hbr[2, at, :].astype(F32)
        sc = scr[at, :]
        sig = jax.nn.sigmoid(gate)
        act = gate * sig
        hc = sc * hb
        cot[at, 0:128] = (hc * up * sig * (1.0 + gate * (1.0 - sig))).astype(BF)
        cot[at, 128:256] = (hc * act).astype(BF)
        rp[at, :] = act * up * hb
        return carry

    lax.fori_loop(0, 4, activate, 0)

    def everyone(buf, ssem, rsem):
        return [
            remote(buf.at[t], buf.at[t], ssem.at[i], rsem.at[i], (ep, k))
            for i, k in enumerate((right, left, far))
        ]

    c_copies = [
        remote(cot.at[half0], cotp, c_s.at[0], c_r.at[0], (ep, one)),
        remote(cot.at[half1], cotq, c_s.at[1], c_r.at[1], (ep, two)),
    ]
    c_copies[0].start()
    lax.fori_loop(4, 8, activate, 0)
    c_copies[1].start()
    ones16 = jnp.ones((16, 128), F32)
    rsum = mm(ones16, rp[...], NT, lax.Precision.HIGHEST)
    rall[t] = rsum[0:8, :]

    def partial(rows, mine_at, near, near_w, p):
        at = pl.ds(pl.multiple_of(mine_at * 512 + p * 256, 256), 256)
        part = mm(cot[rows], wgu[at, :], NT)
        return part + mm(near[...], near_w[p * 256 : (p + 1) * 256, :], NT)

    def away(p):
        top = partial(slice(0, 256), two, cotp, wp[1], p).astype(BF)
        low = partial(slice(256, 512), one, cotq, wq[1], p).astype(BF)
        for k in range(2):
            ts[0, 2 * p + k] = top[:, k * 128 : (k + 1) * 128]
            ts[1, 2 * p + k] = low[:, k * 128 : (k + 1) * 128]

    def kept(p):
        top = partial(slice(0, 256), t, cotp, wp[0], p)
        low = partial(slice(256, 512), t, cotq, wq[0], p)
        for k in range(2):
            own[2 * p + k, 0:256, :] = top[:, k * 128 : (k + 1) * 128]
            own[2 * p + k, 256:512, :] = low[:, k * 128 : (k + 1) * 128]

    def t_copies(p):
        return (
            remote(ts.at[0, p], rsv.at[0, p], s_s.at[p, 0], s_r.at[p, 0], (ep, two)),
            remote(ts.at[1, p], rsv.at[1, p], s_s.at[p, 1], s_r.at[p, 1], (ep, one)),
        )

    def wgrad(j):
        k, h = j // 2, j % 2
        at = pl.ds(pl.multiple_of(j * 256, 256), 256)
        rows = jnp.concatenate([xs[k, 2 * h], xs[k, 2 * h + 1]], axis=1)
        both = mm(rows, cot[...], TN).astype(BF)
        ggb[at, :] = both[:, 0:128]
        gub[at, :] = both[:, 128:256]
        sq = jnp.square(both.astype(F32))
        ng = mm(ones16, sq[:, 0:128], NT, lax.Precision.HIGHEST)
        nu = mm(ones16, sq[:, 128:256], NT, lax.Precision.HIGHEST)
        rnall[t, pl.ds(2 * j, 1), :] = ng[0:1, 0:128]
        rnall[t, pl.ds(2 * j + 1, 1), :] = ng[0:1, 128:256]
        rnall[t, pl.ds(16 + 2 * j, 1), :] = nu[0:1, 0:128]
        rnall[t, pl.ds(17 + 2 * j, 1), :] = nu[0:1, 128:256]

    def wgrads(lo, hi):
        def body(j, carry):
            wgrad(j)
            return carry

        lax.fori_loop(lo, hi, body, 0)

    def reduced(p):
        landed(t_copies(p))
        ret[p, 0:256, :] = (own[p, 0:256, :] + rsv[0, p].astype(F32)).astype(BF)
        ret[p, 256:512, :] = (own[p, 256:512, :] + rsv[1, p].astype(F32)).astype(BF)
        send_group(lambda r: ret.at[p, r], lambda r: back.at[p, r], b_s.at[p], b_r.at[p])
        back[p, mine, :] = ret[p, mine, :]

    def home(src, dst, ssem, rsem):
        for d in (1, 2, 3):
            remote(src.at[pl.ds(d * SEAT, SEAT)], dst.at[seat(grp)], ssem, rsem, (in_z[d - 1], t)).start()

    def combine(p):
        drain(ret.at[p, most], b_r.at[p])
        tokbuf[p] = mm(c01[...], back[p]).astype(BF)
        home(tokbuf.at[p], srcv.at[p], zb_s.at[p], zb_r.at[p])
        srcv[p, seat(grp), :] = tokbuf[p, 0:SEAT, :]

    r_copies = everyone(rall, r_s, r_r)
    begin(r_copies)
    wgrads(0, 3)
    h_near = (
        remote(wha.at[t], wha.at[t], h_s.at[0], h_r.at[0], (ep, right)),
        remote(wha.at[t], wha.at[t], h_s.at[1], h_r.at[1], (ep, left)),
    )
    h_far = (
        remote(wha.at[left, half0], wha.at[left, half0], h_s.at[2], h_r.at[2], (ep, right)),
        remote(wha.at[right, half1], wha.at[right, half1], h_s.at[3], h_r.at[3], (ep, left)),
    )
    begin(h_near)
    landed(swap)
    landed(c_copies)
    away(0)
    begin(t_copies(0))
    away(1)

    landed(r_copies)
    rtot = ((rall[0] + rall[1]) + rall[2]) + rall[3]
    rtot = jnp.where(lax.broadcasted_iota(I32, (8, SLOTS), 0) == 0, rtot, 0.0)
    retr[...] = mm(rtot.astype(BF), jnp.ones((8, 128), BF), TN).astype(BF)
    begin(t_copies(1))
    send_group(lambda r: retr.at[r], lambda r: backr.at[r], br_s, br_r)
    backr[mine, :] = retr[mine, :]
    kept(0)
    begin(t_copies(2))
    landed(h_near)
    begin(h_far)
    reduced(0)
    begin(t_copies(3))
    kept(1)
    reduced(1)

    landed(h_far)
    crows = [jnp.concatenate([cs[0], cs[1]], axis=1), jnp.concatenate([cs[2], cs[3]], axis=1)]

    def dgrad(k, carry):
        for c in range(2):
            gds[k, :, c * 256 : (c + 1) * 256] = mm(wha[k], crows[c], TN).astype(BF)
        return carry

    lax.fori_loop(0, 4, dgrad, 0)
    gdin[t] = gds[t]
    g_copies = [
        remote(gds.at[k], gdin.at[t], v_s.at[i], v_r.at[i], (ep, k))
        for i, k in enumerate((far, right, left))
    ]
    begin(g_copies)
    reduced(2)
    wgrads(3, 5)
    reduced(3)
    combine(0)
    wgrads(5, 8)
    n_copies = everyone(rnall, n_s, n_r)
    begin(n_copies)
    combine(1)
    drain(retr.at[most], br_r)
    lane2 = lax.broadcasted_iota(I32, (RELAY, 128), 1)
    rtb[...] = jnp.where(lane2 == 0, mm(c0[...], backr[...]), mm(c1[...], backr[...])).astype(BF)
    home(rtb, srcr, zr_s, zr_r)
    srcr[seat(grp), :] = rtb[0:SEAT, :]
    landed(n_copies)
    norms = ((rnall[0] + rnall[1]) + rnall[2]) + rnall[3]
    gr_ref[...] = norms[0:16, :]
    ur_ref[...] = norms[16:32, :]
    combine(2)
    combine(3)
    landed(g_copies)
    total = jnp.zeros((128, 128), F32)
    for k in range(4):
        gdr[:, k * 512 : (k + 1) * 512] = gdin[k]
        sq = jnp.square(gdin[k].astype(F32))
        total += sq[:, 0:128] + sq[:, 128:256] + sq[:, 256:384] + sq[:, 384:512]
    dr_ref[...] = mm(ones16, total, NT, lax.Precision.HIGHEST)[0:1, :]

    three = pl.ds(0, 3 * SEAT)

    def finish(p):
        drain(tokbuf.at[p, three], zb_r.at[p])
        tg_ref[:, p * 128 : (p + 1) * 128] = mm(t1[...], srcv[p], TN).astype(BF)

    finish(0)
    finish(1)
    drain(rtb.at[three], zr_r)
    rg_ref[...] = mm(srcr[...], t1[...], TN)[0:2, :].astype(BF)

    drain(sendmeta.at[three], zm_s)
    for i, (q0, n) in enumerate(CHUNKS):
        drain(sendbuf.at[pl.ds(q0, n), three], z_s.at[i])
        drain(pairbuf.at[pl.ds(q0, n), most], y_s.at[i])
    for i in range(4):
        left_here(x_copies(i))
        left_here(f_copies(i))
    drain(scbuf.at[pl.ds(0, GROUP - 1)], ys_s)
    for group in (exch, swap, k_copies, c_copies, h_near, h_far, r_copies, n_copies, g_copies):
        left_here(group)
    for p in range(4):
        left_here(t_copies(p))
        drain(ret.at[p, most], b_s.at[p])
        drain(tokbuf.at[p, three], zb_s.at[p])
    drain(retr.at[most], br_s)
    drain(rtb.at[three], zr_s)
    finish(2)
    finish(3)


def store(*refs):
    sems = refs[16]
    copies = [pltpu.make_async_copy(refs[i], refs[8 + i], sems.at[i]) for i in range(8)]
    for c in copies:
        c.start()
    for c in copies:
        c.wait()


def on_device(tokens, expert_ids, route_weights, cotangent, w_gate, w_up, w_down):
    vmem = pl.BlockSpec(memory_space=pltpu.VMEM)
    hbm = pl.BlockSpec(memory_space=pl.ANY)
    dma = pltpu.SemaphoreType.DMA
    v = pltpu.VMEM
    scratch = [
        v((TOK, 1024), BF),
        v((RELAY, TOK), BF),
        v((8, RELAY, 128), BF),
        v((RELAY, 128), BF),
        v((8, RELAY, 128), BF),
        v((RELAY, 128), BF),
        v((SLOTS, RELAY), BF),
        v((8, SLOTS, 128), BF),
        v((GROUP, 1, 128), F32),
        v((GROUP, 1, 128), F32),
        v((4, 4, SLOTS, 128), BF),
        v((4, SLOTS, 128), BF),
        v((SLOTS, 128), F32),
        v((2048, 256), BF),
        v((4, 128, 512), BF),
        v((2, 512, 256), BF),
        v((2, 512, 256), BF),
        v((SLOTS, 256), F32),
        v((4, SLOTS, 128), F32),
        v((4, SLOTS, 128), BF),
        v((3, SLOTS, 128), BF),
        v((SLOTS, 256), BF),
        v((256, 256), BF),
        v((256, 256), BF),
        v((4, SLOTS, 128), BF),
        v((SLOTS, 128), F32),
        v((4, 8, SLOTS), F32),
        v((2, 4, 256, 128), BF),
        v((2, 4, 256, 128), BF),
        v((4, SLOTS, 128), F32),
        v((4, SLOTS, 128), BF),
        v((SLOTS, 128), BF),
        v((4, SLOTS, 128), BF),
        v((SLOTS, 128), BF),
        v((RELAY, SLOTS), BF),
        v((RELAY, SLOTS), BF),
        v((RELAY, SLOTS), BF),
        v((4, RELAY, 128), BF),
        v((RELAY, 128), BF),
        v((4, RELAY, 128), BF),
        v((RELAY, 128), BF),
        v((4, 128, 512), BF),
        v((4, 128, 512), BF),
        v((4, 32, 128), F32),
        v((2, TOK), I32),
        v((2, TOK), BF),
        dma((4,)), dma((3,)),
        dma((6,)), dma((6,)), dma(()), dma(()),
        dma((6,)), dma((6,)), dma(()), dma(()),
        dma((4, 4)), dma((4, 4)),
        dma((4,)), dma((4,)),
        dma((3,)), dma((3,)),
        dma((3,)), dma((3,)),
        dma((4,)), dma((4,)),
        dma((3,)), dma((3,)),
        dma((2,)), dma((2,)),
        dma((3,)), dma((3,)),
        dma((4, 2)), dma((4, 2)),
        dma((4,)), dma((4,)), dma(()), dma(()),
        dma((4,)), dma((4,)), dma(()), dma(()),
        dma((3,)), dma((3,)),
    ]
    outs = (
        v((TOK, 512), BF), v((2, TOK), BF), v((2048, 128), BF), v((2048, 128), BF),
        v((128, 2048), BF), v((16, 128), F32), v((16, 128), F32), v((1, 128), F32),
    )
    held = pl.pallas_call(
        kernel,
        out_shape=outs,
        in_specs=[hbm] * 7,
        out_specs=(vmem,) * 8,
        scratch_shapes=scratch,
        compiler_params=pltpu.CompilerParams(collective_id=0, has_side_effects=True),
    )(expert_ids.T, route_weights.T, tokens, cotangent, w_gate[0], w_up[0], w_down[0])
    tg, rg, gg, gu, gd, gr, ur, dr = pl.pallas_call(
        store,
        out_shape=tuple(jax.ShapeDtypeStruct(o.shape, o.dtype) for o in outs),
        in_specs=[vmem] * 8,
        out_specs=(hbm,) * 8,
        scratch_shapes=[dma((8,))],
    )(*[pltpu.with_memory_space_constraint(h, pltpu.VMEM) for h in held])
    return (
        tg, rg.T, gg[None], gu[None], gd[None],
        gr.reshape(1, 2048), ur.reshape(1, 2048), dr,
    )


def solution(mesh):
    return jax.shard_map(
        on_device,
        mesh=mesh,
        in_specs=(
            P("ep", None), P("ep", None), P("ep", None), P("ep", None),
            P("ep", None, "tp"), P("ep", None, "tp"), P("ep", "tp", None),
        ),
        out_specs=(
            P("ep", "tp"), P("ep", None), P("ep", None, "tp"), P("ep", None, "tp"),
            P("ep", "tp", None), P("ep", None), P("ep", None), P("ep", "tp"),
        ),
        check_vma=False,
    )
```

```python
import functools

import jax
import jax.numpy as jnp
from jax import lax
from jax.experimental import pallas as pl
from jax.experimental.pallas import tpu as pltpu
from jax.sharding import PartitionSpec as P

MESH = pl.DeviceIdType.MESH
BF = jnp.bfloat16
F32 = jnp.float32
I32 = jnp.int32

PLANES = 8
ROW = 16
GROUP = 32
TOK = 128
SEAT = 64
RELAY = 4 * SEAT
SLOTS = 512
BLK = 16
CHUNKS = ((0, 1), (1, 1), (2, 1), (3, 1), (4, 2), (6, 2))
NN = (((1,), (0,)), ((), ()))
NT = (((1,), (1,)), ((), ()))
TN = (((0,), (0,)), ((), ()))


def mm(a, b, dims=NN, precision=None):
    return lax.dot_general(a, b, dims, precision=precision, preferred_element_type=F32)


def kernel(
    ids_hbm, rw_hbm, tok_hbm, cot_hbm, wg_hbm, wu_hbm, wd_hbm,
    tg_ref, rg_ref, ggb, gub, gdr, gr_ref, ur_ref, dr_ref,
    xc, t1, sendbuf, sendmeta, relay, zmeta, p2, pairbuf, scbuf, scin, xs, cs, scr,
    wgu, wdd, wp, wq, acc_gu, acc_hb, hbp, hbr, cot, cotp, cotq, wha, rp, rall, ts, rsv, own, ret, retr, back, backr, c01, c0, c1,
    tokbuf, rtb, srcv, srcr, gds, gdin, rnall, ids_v, rw_v,
    ld_s, w_s, z_s, z_r, zm_s, zm_r, y_s, y_r, ys_s, ys_r, x_s, x_r, h_s, h_r, v_s, v_r, e_s, e_r, u_s, u_r, k_s, k_r, c_s, c_r,
    r_s, r_r, s_s, s_r, b_s, b_r, br_s, br_r, zb_s, zb_r, zr_s, zr_r, n_s, n_r,
):
    ep = lax.axis_index("ep")
    t = lax.axis_index("tp")
    z = ep // ROW
    yc = ep % ROW
    sg = 1 - 2 * (z % 2)
    grp = z // 2
    base = grp * GROUP
    loc = ep % GROUP
    right = (t + 1) % 4
    left = (t + 3) % 4
    far = (t + 2) % 4
    one = t + 1 - 2 * (t % 2)
    two = 3 - t

    def plane(off):
        return ((z + off + PLANES) % PLANES) * ROW + yc

    out_z = [plane(-sg), plane(2 * sg), plane(-3 * sg)]
    in_z = [plane(-sg), plane(-2 * sg), plane(-3 * sg)]

    def remote(src, dst, ssem, rsem, dev):
        return pltpu.make_async_remote_copy(
            src_ref=src, dst_ref=dst, send_sem=ssem, recv_sem=rsem,
            device_id=dev, device_id_type=MESH,
        )

    def drain(ref, sem):
        pltpu.make_async_copy(ref, ref, sem).wait()

    def begin(copies):
        for c in copies:
            c.start()

    def landed(copies):
        for c in copies:
            c.wait_recv()

    def left_here(copies):
        for c in copies:
            c.wait_send()

    def peer(o):
        return (loc + o) % GROUP

    def rows16(i):
        return pl.ds(pl.multiple_of(i * BLK, BLK), BLK)

    def seat(i):
        return pl.ds(pl.multiple_of(i * SEAT, SEAT), SEAT)

    def block(k):
        return pl.ds(pl.multiple_of(k * 512, 512), 512)

    barrier = pltpu.get_barrier_semaphore()

    def hello(e, k):
        pl.semaphore_signal(barrier, inc=1, device_id=(e, k), device_id_type=MESH)

    for e in (plane(-3 * sg), plane(2), plane(-2), plane(-sg)):
        hello(e, t)

    route_in = [
        pltpu.make_async_copy(ids_hbm, ids_v, ld_s.at[2]),
        pltpu.make_async_copy(rw_hbm, rw_v, ld_s.at[3]),
    ]
    begin(route_in)
    ld = [
        pltpu.make_async_copy(tok_hbm.at[:, block(t)], xc.at[:, pl.ds(0, 512)], ld_s.at[0]),
        pltpu.make_async_copy(cot_hbm.at[:, block(t)], xc.at[:, pl.ds(512, 512)], ld_s.at[1]),
    ]
    wl = [
        pltpu.make_async_copy(wg_hbm, wgu.at[:, pl.ds(0, 128)], w_s.at[0]),
        pltpu.make_async_copy(wu_hbm, wgu.at[:, pl.ds(128, 128)], w_s.at[1]),
        pltpu.make_async_copy(wd_hbm.at[:, block(t)], wdd.at[t], w_s.at[2]),
    ]
    begin(ld)

    for k in (far, right, left):
        hello(ep, k)

    def hello_group(o, carry):
        hello(base + peer(o), t)
        return carry

    lax.fori_loop(1, GROUP, hello_group, 0)

    for c in route_in:
        c.wait()
    ids = ids_v[...]
    id0, id1 = ids[0:1, :], ids[1:2, :]
    sub = lax.broadcasted_iota(I32, (TOK, TOK), 0)
    lane = lax.broadcasted_iota(I32, (TOK, TOK), 1)
    oh0 = jnp.where(sub == id0, 1.0, 0.0)
    oh1 = jnp.where(sub == id1, 1.0, 0.0)
    upper = jnp.where(sub < lane, 1.0, 0.0).astype(BF)
    before = mm((oh0 + oh1).astype(BF), upper)
    k0 = jnp.sum(before * oh0, axis=0, keepdims=True)
    k1 = jnp.sum(before * oh1, axis=0, keepdims=True)
    g = id0 // GROUP
    ohg = jnp.where(lax.broadcasted_iota(I32, (16, TOK), 0) == g, 1.0, 0.0)
    q = jnp.sum(mm(ohg.astype(BF), upper) * ohg, axis=0, keepdims=True)
    slot = g * SEAT + q.astype(I32)
    code0 = ((id0 - g * GROUP) * 4).astype(F32) + k0
    code1 = ((id1 - g * GROUP) * 4).astype(F32) + k1
    rw = rw_v[...].astype(F32)
    mrow = jnp.where(
        sub == 0, code0,
        jnp.where(sub == 1, code1, jnp.where(sub == 2, rw[0:1, :], jnp.where(sub == 3, rw[1:2, :], 0.0))),
    ).astype(BF)
    t1[...] = jnp.where(lax.broadcasted_iota(I32, (RELAY, TOK), 0) == slot, 1.0, 0.0).astype(BF)
    sendmeta[...] = mm(t1[...], mrow, NT).astype(BF)
    for c in ld:
        c.wait()
    for h in range(4):
        part = mm(t1[...], xc[:, h * 256 : (h + 1) * 256]).astype(BF)
        sendbuf[2 * h] = part[:, 0:128]
        sendbuf[2 * h + 1] = part[:, 128:256]

    pl.semaphore_wait(barrier, 3 + 4 + GROUP - 1)

    def send_meta():
        for d in (1, 2, 3):
            dst = out_z[d - 1]
            here = pl.ds(d * SEAT, SEAT)
            remote(sendmeta.at[seat(dst // GROUP)], zmeta.at[here], zm_s, zm_r, (dst, t)).start()

    def send_z(i):
        qs = pl.ds(*CHUNKS[i])
        for d in (1, 2, 3):
            dst = out_z[d - 1]
            here = pl.ds(d * SEAT, SEAT)
            remote(
                sendbuf.at[qs, seat(dst // GROUP)], relay.at[qs, here], z_s.at[i], z_r.at[i], (dst, t)
            ).start()

    exch = [
        remote(wd_hbm.at[:, block(k)], wdd.at[t], e_s.at[i], e_r.at[i], (ep, k))
        for i, k in enumerate((right, left, far))
    ]
    send_meta()
    send_z(0)
    send_z(1)
    begin(wl)
    begin(exch)
    zmeta[0:SEAT, :] = sendmeta[seat(grp), :]
    for h in range(8):
        relay[h, 0:SEAT, :] = sendbuf[h, seat(grp), :]
    for c in wl:
        c.wait()
    swap = [
        remote(wgu.at[block(two)], wq.at[0], u_s.at[0], u_r.at[0], (ep, two)),
        remote(wgu.at[block(one)], wp.at[0], u_s.at[1], u_r.at[1], (ep, one)),
        remote(wgu.at[block(far)], wq.at[1], u_s.at[2], u_r.at[2], (ep, two)),
        remote(wgu.at[block(far)], wp.at[1], u_s.at[3], u_r.at[3], (ep, one)),
    ]
    begin(swap)

    drain(zmeta.at[pl.ds(SEAT, 3 * SEAT)], zm_r)
    send_z(2)
    pick = jnp.where(
        lax.broadcasted_iota(I32, (16, 128), 0) == lax.broadcasted_iota(I32, (16, 128), 1), 1.0, 0.0
    ).astype(BF)
    flat = mm(pick, zmeta[...], NT)
    seatrow = lax.broadcasted_iota(I32, (1, RELAY), 1) // SEAT

    def place(code, where_seat):
        code = code.astype(I32)
        return (code // 4) * BLK + where_seat * 4 + code % 4

    pos0 = place(flat[0:1, :], seatrow)
    pos1 = place(flat[1:2, :], seatrow)

    def spread(i, carry):
        at = pl.ds(pl.multiple_of(i * 128, 128), 128)
        p = lax.broadcasted_iota(I32, (128, RELAY), 0) + i * 128
        e0, e1 = p == pos0, p == pos1
        p2[at, :] = jnp.where(e0, 1.0, jnp.where(e1, 1.0, 0.0)).astype(BF)
        return carry

    lax.fori_loop(0, 4, spread, 0)

    def send_group(src, dst, ssem, rsem):
        def body(o, carry):
            e = peer(o)
            remote(src(rows16(e)), dst(rows16(loc)), ssem, rsem, (base + e, t)).start()
            return carry

        lax.fori_loop(1, GROUP, body, 0)

    mine = rows16(loc)
    most = pl.ds(0, (GROUP - 1) * BLK)

    def relay_step(i):
        q0, n = CHUNKS[i]
        drain(relay.at[pl.ds(q0, n), pl.ds(SEAT, 3 * SEAT)], z_r.at[i])
        rows = relay[q0] if n == 1 else jnp.concatenate([relay[q0], relay[q0 + 1]], axis=1)
        out = mm(p2[...], rows).astype(BF)
        for k in range(n):
            pairbuf[q0 + k] = out[:, k * 128 : (k + 1) * 128]
        qs = pl.ds(q0, n)
        if q0 < 4:
            send_group(
                lambda r: pairbuf.at[qs, r], lambda r: xs.at[t, qs, r], y_s.at[i], y_r.at[i]
            )
            for k in range(n):
                xs[t, q0 + k, mine, :] = pairbuf[q0 + k, mine, :]
        else:
            qc = pl.ds(q0 - 4, n)
            send_group(
                lambda r: pairbuf.at[qs, r], lambda r: cs.at[qc, r], y_s.at[i], y_r.at[i]
            )
            for k in range(n):
                cs[q0 - 4 + k, mine, :] = pairbuf[q0 + k, mine, :]

    def routed(i):
        drain(pairbuf.at[pl.ds(*CHUNKS[i]), most], y_r.at[i])

    half0, half1 = pl.ds(0, 256), pl.ds(256, 256)

    def x_copies(i):
        qs = pl.ds(*CHUNKS[i])
        return (
            remote(xs.at[t, qs], xs.at[t, qs], x_s.at[i, 0], x_r.at[i, 0], (ep, right)),
            remote(xs.at[t, qs], xs.at[t, qs], x_s.at[i, 1], x_r.at[i, 1], (ep, left)),
        )

    def f_copies(i):
        qs = pl.ds(*CHUNKS[i])
        return (
            remote(xs.at[left, qs, half0], xs.at[left, qs, half0], x_s.at[i, 2], x_r.at[i, 2], (ep, right)),
            remote(xs.at[right, qs, half1], xs.at[right, qs, half1], x_s.at[i, 3], x_r.at[i, 3], (ep, left)),
        )

    def forward_step(i):
        landed(x_copies(i))
        begin(f_copies(i))

    def product(k, i, first=False):
        q0, n = CHUNKS[i]
        at = pl.ds(pl.multiple_of(k * 512 + q0 * 128, 128), n * 128)
        rows = xs[k, q0] if n == 1 else jnp.concatenate([xs[k, q0], xs[k, q0 + 1]], axis=1)
        part = mm(rows, wgu[at, :])
        if first:
            acc_gu[...] = part
        else:
            acc_gu[...] += part

    def near_products(i):
        def body(j, carry):
            product((t + 1 + 2 * j) % 4, i)
            return carry

        lax.fori_loop(0, 2, body, 0)

    def hb_rows(c):
        return jnp.concatenate([cs[2 * c], cs[2 * c + 1]], axis=1)

    def hb_start():
        rows = hb_rows(0)

        def body(k, carry):
            acc_hb[k] = mm(rows, wdd[k, :, 0:256], NT)
            return carry

        lax.fori_loop(0, 4, body, 0)

    def hb_whole(k):
        return acc_hb[k] + mm(hb_rows(1), wdd[k, :, 256:512], NT)

    relay_step(0)
    relay_step(1)
    send_z(3)
    send_z(4)
    routed(0)
    begin(x_copies(0))
    product(t, 0, first=True)
    relay_step(2)
    send_z(5)

    seatcol = lax.broadcasted_iota(I32, (RELAY, 1), 0) // SEAT
    codes = zmeta[...].astype(F32)
    lanes = lax.broadcasted_iota(I32, (RELAY, 128), 1)

    def weight_rows(k):
        code = codes[:, k : k + 1].astype(I32)
        to = jnp.where(lanes == code // 4, 1.0, 0.0).astype(BF)
        at = jnp.where(lanes == seatcol * 4 + code % 4, codes[:, k + 2 : k + 3], 0.0).astype(BF)
        return mm(to, at, TN)

    table = weight_rows(0) + weight_rows(1)
    for e in range(GROUP):
        scbuf[e] = table[e : e + 1, :]

    def send_weights(o, carry):
        e = peer(o)
        remote(scbuf.at[e], scin.at[loc], ys_s, ys_r, (base + e, t)).start()
        return carry

    lax.fori_loop(1, GROUP, send_weights, 0)
    scin[loc] = scbuf[loc]
    routed(1)
    begin(x_copies(1))
    product(t, 1)
    relay_step(3)
    relay_step(4)
    routed(2)
    begin(x_copies(2))
    product(t, 2)
    forward_step(0)
    relay_step(5)
    near_products(0)
    routed(3)
    begin(x_copies(3))
    product(t, 3)

    back0 = place(codes[:, 0:1], seatcol)
    back1 = place(codes[:, 1:2], seatcol)
    wide = lax.broadcasted_iota(I32, (RELAY, SLOTS), 1)
    m0 = jnp.where(wide == back0, 1.0, 0.0)
    m1 = jnp.where(wide == back1, 1.0, 0.0)
    c0[...] = m0.astype(BF)
    c1[...] = m1.astype(BF)
    c01[...] = (m0 + m1).astype(BF)

    forward_step(1)
    near_products(1)
    landed(exch)
    forward_step(2)
    near_products(2)
    routed(4)
    hb_start()
    landed(f_copies(0))
    product(far, 0)
    forward_step(3)
    routed(5)
    k_copies = [
        remote(hbp.at[k], hbr.at[i], k_s.at[i], k_r.at[i], (ep, k))
        for i, k in enumerate((far, right, left))
    ]
    for i, k in enumerate((far, right, left)):
        hbp[k] = hb_whole(k).astype(BF)
        k_copies[i].start()
    acc_hb[t] = hb_whole(t)
    near_products(3)
    for i in (1, 2, 3):
        landed(f_copies(i))
        product(far, i)

    drain(scbuf.at[pl.ds(0, GROUP - 1)], ys_r)
    prow = lax.broadcasted_iota(I32, (SLOTS, GROUP), 0)
    from_relay = jnp.where(prow // BLK == lax.broadcasted_iota(I32, (SLOTS, GROUP), 1), 1.0, 0.0)
    listed = mm(from_relay.astype(BF), scin[:, 0, :].astype(BF))
    inside = lax.broadcasted_iota(I32, (SLOTS, 128), 0) % BLK == lax.broadcasted_iota(I32, (SLOTS, 128), 1)
    scr[...] = mm(jnp.where(inside, listed, 0.0).astype(BF), jnp.ones((128, 128), BF))

    def hiddens(i, carry):
        at = pl.ds(pl.multiple_of(i * 64, 64), 64)
        gate, up = acc_gu[at, 0:128], acc_gu[at, 128:256]
        hid = gate * jax.nn.sigmoid(gate) * up
        wha[t, at, :] = (scr[at, :] * hid).astype(BF)
        return carry

    lax.fori_loop(0, 8, hiddens, 0)
    landed(k_copies)

    def activate(i, carry):
        at = pl.ds(pl.multiple_of(i * 64, 64), 64)
        gate, up = acc_gu[at, 0:128], acc_gu[at, 128:256]
        hb = acc_hb[t, at, :] + hbr[0, at, :].astype(F32)
        hb = hb + hbr[1, at, :].astype(F32) + hbr[2, at, :].astype(F32)
        sc = scr[at, :]
        sig = jax.nn.sigmoid(gate)
        act = gate * sig
        hc = sc * hb
        cot[at, 0:128] = (hc * up * sig * (1.0 + gate * (1.0 - sig))).astype(BF)
        cot[at, 128:256] = (hc * act).astype(BF)
        rp[at, :] = act * up * hb
        return carry

    lax.fori_loop(0, 4, activate, 0)

    def everyone(buf, ssem, rsem):
        return [
            remote(buf.at[t], buf.at[t], ssem.at[i], rsem.at[i], (ep, k))
            for i, k in enumerate((right, left, far))
        ]

    c_copies = [
        remote(cot.at[half0], cotp, c_s.at[0], c_r.at[0], (ep, one)),
        remote(cot.at[half1], cotq, c_s.at[1], c_r.at[1], (ep, two)),
    ]
    c_copies[0].start()
    lax.fori_loop(4, 8, activate, 0)
    c_copies[1].start()
    ones16 = jnp.ones((16, 128), F32)
    rsum = mm(ones16, rp[...], NT, lax.Precision.HIGHEST)
    rall[t] = rsum[0:8, :]

    def partial(rows, mine_at, near, near_w, p):
        at = pl.ds(pl.multiple_of(mine_at * 512 + p * 256, 256), 256)
        part = mm(cot[rows], wgu[at, :], NT)
        return part + mm(near[...], near_w[p * 256 : (p + 1) * 256, :], NT)

    def away(p):
        top = partial(slice(0, 256), two, cotp, wp[1], p).astype(BF)
        low = partial(slice(256, 512), one, cotq, wq[1], p).astype(BF)
        for k in range(2):
            ts[0, 2 * p + k] = top[:, k * 128 : (k + 1) * 128]
            ts[1, 2 * p + k] = low[:, k * 128 : (k + 1) * 128]

    def kept(p):
        top = partial(slice(0, 256), t, cotp, wp[0], p)
        low = partial(slice(256, 512), t, cotq, wq[0], p)
        for k in range(2):
            own[2 * p + k, 0:256, :] = top[:, k * 128 : (k + 1) * 128]
            own[2 * p + k, 256:512, :] = low[:, k * 128 : (k + 1) * 128]

    def t_copies(p):
        return (
            remote(ts.at[0, p], rsv.at[0, p], s_s.at[p, 0], s_r.at[p, 0], (ep, two)),
            remote(ts.at[1, p], rsv.at[1, p], s_s.at[p, 1], s_r.at[p, 1], (ep, one)),
        )

    def wgrad(j):
        k, h = j // 2, j % 2
        at = pl.ds(pl.multiple_of(j * 256, 256), 256)
        rows = jnp.concatenate([xs[k, 2 * h], xs[k, 2 * h + 1]], axis=1)
        both = mm(rows, cot[...], TN).astype(BF)
        ggb[at, :] = both[:, 0:128]
        gub[at, :] = both[:, 128:256]
        sq = jnp.square(both.astype(F32))
        ng = mm(ones16, sq[:, 0:128], NT, lax.Precision.HIGHEST)
        nu = mm(ones16, sq[:, 128:256], NT, lax.Precision.HIGHEST)
        rnall[t, pl.ds(2 * j, 1), :] = ng[0:1, 0:128]
        rnall[t, pl.ds(2 * j + 1, 1), :] = ng[0:1, 128:256]
        rnall[t, pl.ds(16 + 2 * j, 1), :] = nu[0:1, 0:128]
        rnall[t, pl.ds(17 + 2 * j, 1), :] = nu[0:1, 128:256]

    def wgrads(lo, hi):
        def body(j, carry):
            wgrad(j)
            return carry

        lax.fori_loop(lo, hi, body, 0)

    def reduced(p):
        landed(t_copies(p))
        ret[p, 0:256, :] = (own[p, 0:256, :] + rsv[0, p].astype(F32)).astype(BF)
        ret[p, 256:512, :] = (own[p, 256:512, :] + rsv[1, p].astype(F32)).astype(BF)
        send_group(lambda r: ret.at[p, r], lambda r: back.at[p, r], b_s.at[p], b_r.at[p])
        back[p, mine, :] = ret[p, mine, :]

    def home(src, dst, ssem, rsem):
        for d in (1, 2, 3):
            remote(src.at[pl.ds(d * SEAT, SEAT)], dst.at[seat(grp)], ssem, rsem, (in_z[d - 1], t)).start()

    def combine(p):
        drain(ret.at[p, most], b_r.at[p])
        tokbuf[p] = mm(c01[...], back[p]).astype(BF)
        home(tokbuf.at[p], srcv.at[p], zb_s.at[p], zb_r.at[p])
        srcv[p, seat(grp), :] = tokbuf[p, 0:SEAT, :]

    r_copies = everyone(rall, r_s, r_r)
    begin(r_copies)
    wgrads(0, 3)
    h_near = (
        remote(wha.at[t], wha.at[t], h_s.at[0], h_r.at[0], (ep, right)),
        remote(wha.at[t], wha.at[t], h_s.at[1], h_r.at[1], (ep, left)),
    )
    h_far = (
        remote(wha.at[left, half0], wha.at[left, half0], h_s.at[2], h_r.at[2], (ep, right)),
        remote(wha.at[right, half1], wha.at[right, half1], h_s.at[3], h_r.at[3], (ep, left)),
    )
    begin(h_near)
    landed(swap)
    landed(c_copies)
    away(0)
    begin(t_copies(0))
    away(1)

    landed(r_copies)
    rtot = ((rall[0] + rall[1]) + rall[2]) + rall[3]
    rtot = jnp.where(lax.broadcasted_iota(I32, (8, SLOTS), 0) == 0, rtot, 0.0)
    retr[...] = mm(rtot.astype(BF), jnp.ones((8, 128), BF), TN).astype(BF)
    begin(t_copies(1))
    send_group(lambda r: retr.at[r], lambda r: backr.at[r], br_s, br_r)
    backr[mine, :] = retr[mine, :]
    kept(0)
    begin(t_copies(2))
    landed(h_near)
    begin(h_far)
    reduced(0)
    begin(t_copies(3))
    kept(1)
    reduced(1)

    landed(h_far)
    crows = [jnp.concatenate([cs[0], cs[1]], axis=1), jnp.concatenate([cs[2], cs[3]], axis=1)]

    def dgrad(k, carry):
        for c in range(2):
            gds[k, :, c * 256 : (c + 1) * 256] = mm(wha[k], crows[c], TN).astype(BF)
        return carry

    lax.fori_loop(0, 4, dgrad, 0)
    gdin[t] = gds[t]
    g_copies = [
        remote(gds.at[k], gdin.at[t], v_s.at[i], v_r.at[i], (ep, k))
        for i, k in enumerate((far, right, left))
    ]
    begin(g_copies)
    reduced(2)
    wgrads(3, 5)
    reduced(3)
    combine(0)
    wgrads(5, 8)
    n_copies = everyone(rnall, n_s, n_r)
    begin(n_copies)
    combine(1)
    drain(retr.at[most], br_r)
    lane2 = lax.broadcasted_iota(I32, (RELAY, 128), 1)
    rtb[...] = jnp.where(lane2 == 0, mm(c0[...], backr[...]), mm(c1[...], backr[...])).astype(BF)
    home(rtb, srcr, zr_s, zr_r)
    srcr[seat(grp), :] = rtb[0:SEAT, :]
    combine(2)
    combine(3)
    landed(n_copies)
    norms = ((rnall[0] + rnall[1]) + rnall[2]) + rnall[3]
    gr_ref[...] = norms[0:16, :]
    ur_ref[...] = norms[16:32, :]
    landed(g_copies)
    total = jnp.zeros((128, 128), F32)
    for k in range(4):
        gdr[:, k * 512 : (k + 1) * 512] = gdin[k]
        sq = jnp.square(gdin[k].astype(F32))
        total += sq[:, 0:128] + sq[:, 128:256] + sq[:, 256:384] + sq[:, 384:512]
    dr_ref[...] = mm(ones16, total, NT, lax.Precision.HIGHEST)[0:1, :]

    three = pl.ds(0, 3 * SEAT)

    def finish(p):
        drain(tokbuf.at[p, three], zb_r.at[p])
        tg_ref[:, p * 128 : (p + 1) * 128] = mm(t1[...], srcv[p], TN).astype(BF)

    finish(0)
    finish(1)
    drain(rtb.at[three], zr_r)
    rg_ref[...] = mm(srcr[...], t1[...], TN)[0:2, :].astype(BF)

    drain(sendmeta.at[three], zm_s)
    for i, (q0, n) in enumerate(CHUNKS):
        drain(sendbuf.at[pl.ds(q0, n), three], z_s.at[i])
        drain(pairbuf.at[pl.ds(q0, n), most], y_s.at[i])
    for i in range(4):
        left_here(x_copies(i))
        left_here(f_copies(i))
    drain(scbuf.at[pl.ds(0, GROUP - 1)], ys_s)
    for group in (exch, swap, k_copies, c_copies, h_near, h_far, r_copies, n_copies, g_copies):
        left_here(group)
    for p in range(4):
        left_here(t_copies(p))
        drain(ret.at[p, most], b_s.at[p])
        drain(tokbuf.at[p, three], zb_s.at[p])
    drain(retr.at[most], br_s)
    drain(rtb.at[three], zr_s)
    finish(2)
    finish(3)


def store(*refs):
    sems = refs[16]
    copies = [pltpu.make_async_copy(refs[i], refs[8 + i], sems.at[i]) for i in range(8)]
    for c in copies:
        c.start()
    for c in copies:
        c.wait()


def on_device(tokens, expert_ids, route_weights, cotangent, w_gate, w_up, w_down):
    vmem = pl.BlockSpec(memory_space=pltpu.VMEM)
    hbm = pl.BlockSpec(memory_space=pl.ANY)
    dma = pltpu.SemaphoreType.DMA
    v = pltpu.VMEM
    scratch = [
        v((TOK, 1024), BF),
        v((RELAY, TOK), BF),
        v((8, RELAY, 128), BF),
        v((RELAY, 128), BF),
        v((8, RELAY, 128), BF),
        v((RELAY, 128), BF),
        v((SLOTS, RELAY), BF),
        v((8, SLOTS, 128), BF),
        v((GROUP, 1, 128), F32),
        v((GROUP, 1, 128), F32),
        v((4, 4, SLOTS, 128), BF),
        v((4, SLOTS, 128), BF),
        v((SLOTS, 128), F32),
        v((2048, 256), BF),
        v((4, 128, 512), BF),
        v((2, 512, 256), BF),
        v((2, 512, 256), BF),
        v((SLOTS, 256), F32),
        v((4, SLOTS, 128), F32),
        v((4, SLOTS, 128), BF),
        v((3, SLOTS, 128), BF),
        v((SLOTS, 256), BF),
        v((256, 256), BF),
        v((256, 256), BF),
        v((4, SLOTS, 128), BF),
        v((SLOTS, 128), F32),
        v((4, 8, SLOTS), F32),
        v((2, 4, 256, 128), BF),
        v((2, 4, 256, 128), BF),
        v((4, SLOTS, 128), F32),
        v((4, SLOTS, 128), BF),
        v((SLOTS, 128), BF),
        v((4, SLOTS, 128), BF),
        v((SLOTS, 128), BF),
        v((RELAY, SLOTS), BF),
        v((RELAY, SLOTS), BF),
        v((RELAY, SLOTS), BF),
        v((4, RELAY, 128), BF),
        v((RELAY, 128), BF),
        v((4, RELAY, 128), BF),
        v((RELAY, 128), BF),
        v((4, 128, 512), BF),
        v((4, 128, 512), BF),
        v((4, 32, 128), F32),
        v((2, TOK), I32),
        v((2, TOK), BF),
        dma((4,)), dma((3,)),
        dma((6,)), dma((6,)), dma(()), dma(()),
        dma((6,)), dma((6,)), dma(()), dma(()),
        dma((4, 4)), dma((4, 4)),
        dma((4,)), dma((4,)),
        dma((3,)), dma((3,)),
        dma((3,)), dma((3,)),
        dma((4,)), dma((4,)),
        dma((3,)), dma((3,)),
        dma((2,)), dma((2,)),
        dma((3,)), dma((3,)),
        dma((4, 2)), dma((4, 2)),
        dma((4,)), dma((4,)), dma(()), dma(()),
        dma((4,)), dma((4,)), dma(()), dma(()),
        dma((3,)), dma((3,)),
    ]
    outs = (
        v((TOK, 512), BF), v((2, TOK), BF), v((2048, 128), BF), v((2048, 128), BF),
        v((128, 2048), BF), v((16, 128), F32), v((16, 128), F32), v((1, 128), F32),
    )
    held = pl.pallas_call(
        kernel,
        out_shape=outs,
        in_specs=[hbm] * 7,
        out_specs=(vmem,) * 8,
        scratch_shapes=scratch,
        compiler_params=pltpu.CompilerParams(collective_id=0, has_side_effects=True),
    )(expert_ids.T, route_weights.T, tokens, cotangent, w_gate[0], w_up[0], w_down[0])
    tg, rg, gg, gu, gd, gr, ur, dr = pl.pallas_call(
        store,
        out_shape=tuple(jax.ShapeDtypeStruct(o.shape, o.dtype) for o in outs),
        in_specs=[vmem] * 8,
        out_specs=(hbm,) * 8,
        scratch_shapes=[dma((8,))],
    )(*[pltpu.with_memory_space_constraint(h, pltpu.VMEM) for h in held])
    return (
        tg, rg.T, gg[None], gu[None], gd[None],
        gr.reshape(1, 2048), ur.reshape(1, 2048), dr,
    )


def solution(mesh):
    return jax.shard_map(
        on_device,
        mesh=mesh,
        in_specs=(
            P("ep", None), P("ep", None), P("ep", None), P("ep", None),
            P("ep", None, "tp"), P("ep", None, "tp"), P("ep", "tp", None),
        ),
        out_specs=(
            P("ep", "tp"), P("ep", None), P("ep", None, "tp"), P("ep", None, "tp"),
            P("ep", "tp", None), P("ep", None), P("ep", None), P("ep", "tp"),
        ),
        check_vma=False,
    )
```
